512 devices in a mesh: sp: 64 (over z, y), tp: 8 (over x, core).
Axes of the slice: x: 4, y: 8, z: 8, core: 2. Of those that a mesh axis runs over, the one named last changes fastest.
Arguments:
- stream: bfloat16 [24576, 2048], P('sp', 'tp'), may hold values from -6 to 6
- norm_gain: float32 [2, 2048], replicated, may hold values from 0.1 to 1.9
- a_weight: bfloat16 [2, 2048, 2048], P(None, 'sp', 'tp'), may hold values from -0.125 to 0.125
- gate_weight: bfloat16 [2, 2048, 2048], P(None, 'sp', 'tp'), may hold values from -0.125 to 0.125
- conv_weight: float32 [2, 31, 2048], P(None, None, 'tp'), may hold values from -4 to 4, as said below
- conv_bias: float32 [2, 2048], P(None, 'tp'), may hold values from -3 to 3
- ln_gain: float32 [2, 2048], P(None, 'tp'), may hold values from 0.1 to 1.9
- ln_shift: float32 [2, 2048], P(None, 'tp'), may hold values from -3 to 3
- out_weight: bfloat16 [2, 2048, 2048], P(None, 'sp', 'tp'), may hold values from -0.125 to 0.125
Outputs:
- result: bfloat16 [24576, 2048], P('sp', 'tp')
The draws below stay inside these ranges and needn't reach their ends.
Inputs may be any that keep to these rules, and one draw needn't show every extreme that they name: `conv_weight`: each column is drawn with its own scale, and blocks of 16 channels differ in scale by up to a factor of nine.
All inputs are finite; a program needn't handle non-finite values.
Results may differ from the reference program's by a relative error of at most 0.01.
Values may be sent and summed in bfloat16 or wider, within the bound.
A program may use at most 64 MiB of HBM per device.

```python
import jax
import jax.numpy as jnp
from jax import lax

D = 2048
WIDTH = 31
LAYERS = 2
TOKENS = 24576


def draw_conv_weight(key, part):
    first = jax.random.fold_in(key, 11)
    second = jax.random.fold_in(key, 12)
    values = jnp.clip(jax.random.normal(first, (LAYERS, WIDTH, D), jnp.float32), -6.0, 6.0)
    block_scale = jnp.exp(jax.random.uniform(second, (LAYERS, 1, D // 16), jnp.float32, -1.09, 1.09))
    spread_scale = jnp.repeat(block_scale, 16, axis=2)
    return values * spread_scale * WIDTH ** (-0.5)


def shard_levels(key, shape, cuts, smallest, high):
    level = 1.0
    for dim, blocks in cuts:
        steps = jax.random.uniform(jax.random.fold_in(jax.random.fold_in(key, 6), dim), (blocks,), jnp.float32, smallest / len(cuts), high / len(cuts))
        level = level * jnp.repeat(jnp.exp(steps), shape[dim] // blocks).reshape((-1,) + (1,) * (len(shape) - 1 - dim))
    return level


def normal_values(stream_key, dims, spread, most, shards=(), kind=jnp.bfloat16):
    drawn = jax.random.normal(stream_key, dims, jnp.float32) * spread
    if len(shards) > 0:
        drawn = shard_levels(stream_key, dims, shards, -0.22, 0.18) * drawn
    return jnp.clip(drawn, min=-most, max=most).astype(kind)


def setup_inputs(seed: int = 0) -> dict:
    arg_keys = jax.random.split(jax.random.key(seed), 10)
    return {
        "stream": normal_values(arg_keys[0], (TOKENS, D), 1.0, 6.0, ((0, 64), (1, 8))),
        "norm_gain": jnp.clip(1.0 + 0.18 * jax.random.normal(arg_keys[1], (LAYERS, D), jnp.float32), 0.1, 1.9),
        "a_weight": normal_values(arg_keys[2], (LAYERS, D, D), D ** -0.5, 0.125, ((1, 64), (2, 8))),
        "gate_weight": normal_values(arg_keys[3], (LAYERS, D, D), D ** -0.5, 0.125, ((1, 64), (2, 8))),
        "conv_weight": draw_conv_weight(jax.random.fold_in(arg_keys[9], 71), 0),
        "conv_bias": normal_values(arg_keys[5], (LAYERS, D), 0.5, 3.0, ((1, 8),), jnp.float32),
        "ln_gain": jnp.clip(1.0 + 0.18 * jax.random.normal(arg_keys[6], (LAYERS, D), jnp.float32), 0.1, 1.9),
        "ln_shift": normal_values(arg_keys[7], (LAYERS, D), 0.5, 3.0, ((1, 8),), jnp.float32),
        "out_weight": normal_values(arg_keys[8], (LAYERS, D, D), D ** -0.5, 0.125, ((1, 64), (2, 8))),
    }


EPSILON = 1e-06

def normalize_rows(stream_f, gain):
    factor = lax.rsqrt(lax.optimization_barrier(jnp.mean(stream_f * stream_f, axis=1, keepdims=True)) + EPSILON)
    return (stream_f * factor * gain[None, :]).astype(jnp.bfloat16)

def convolve(padded, kernel, conv_shift, out_rows):
    summed = jnp.zeros((out_rows, padded.shape[1]), jnp.float32) + conv_shift[None, :]
    for offset in range(kernel.shape[0]):
        window = lax.slice_in_dim(padded, offset, offset + out_rows, axis=0).astype(jnp.float32)
        summed = summed + window * kernel[offset][None, :]
    return summed

def finish_norm(conv_out, row_sum, row_squares, gain, shift):
    average = row_sum / D
    variance = row_squares / D - average * average
    normed = (conv_out - average) * lax.rsqrt(variance + EPSILON) * gain[None, :] + shift[None, :]
    return jax.nn.silu(normed).astype(jnp.bfloat16)

def reference(stream, norm_gain, a_weight, gate_weight, conv_weight, conv_bias, ln_gain, ln_shift, out_weight):
    reach = (WIDTH - 1) // 2
    current = stream
    for layer_index in range(LAYERS):
        stream_f = current.astype(jnp.float32)
        normed = normalize_rows(stream_f, norm_gain[layer_index])
        linear = jnp.dot(normed, a_weight[layer_index], preferred_element_type=jnp.float32)
        gating = jnp.dot(normed, gate_weight[layer_index], preferred_element_type=jnp.float32)
        gated = (linear * jax.nn.sigmoid(gating)).astype(jnp.bfloat16)
        padded = jnp.pad(gated, ((reach, reach), (0, 0)))
        conv_out = convolve(padded, conv_weight[layer_index], conv_bias[layer_index], TOKENS)
        row_sum = lax.optimization_barrier(jnp.sum(conv_out, axis=1, keepdims=True))
        row_squares = lax.optimization_barrier(jnp.sum(conv_out * conv_out, axis=1, keepdims=True))
        mixed_in = finish_norm(conv_out, row_sum, row_squares, ln_gain[layer_index], ln_shift[layer_index])
        branch = jnp.dot(mixed_in, out_weight[layer_index], preferred_element_type=jnp.float32)
        current = (stream_f + branch).astype(jnp.bfloat16)
    return current
```

```python
import functools

import jax
import jax.numpy as jnp
from jax import lax
from jax.experimental import pallas as pl
from jax.experimental.pallas import tpu as pltpu
from jax.sharding import PartitionSpec as P

EPSILON = 1e-06
MESH = pl.DeviceIdType.MESH
C = 256
HALO = 32
BLK = 32
SUB = (2, 1, 2, 1)
ITEMS = [(st, h) for st in range(4) for h in range(SUB[st])]


def remote(src, dst, ssem, rsem, dev):
    return pltpu.make_async_remote_copy(
        src_ref=src, dst_ref=dst, send_sem=ssem, recv_sem=rsem, device_id=dev, device_id_type=MESH
    )


def kernel(
    nz, ny, nx, tokens, width,
    stream, a_w, g_w, o_w, norm_gain, conv_w, conv_b, ln_gain, ln_shift,
    out,
    wag, wo, xb0, xb1, mb0, mb1, u, gs, acc, ss, st, so, sb, q, qt, lno, lnb,
    p1_s, p1_r, rg_s, rg_r, xg_s, xg_r, dd_s, dd_r, do_s, do_r, hl_s, hl_r, st_s, st_r, ln_s, ln_r, loc,
):
    tp = 2 * nx
    sp_n = nz * ny
    d_model = C * tp
    kb = d_model // sp_n
    sp = lax.axis_index("sp")
    me = lax.axis_index("tp")
    z, y = sp // ny, lax.rem(sp, ny)
    x, core = me // 2, lax.rem(me, 2)
    sib = me + 1 - 2 * core
    r0, r1, r2 = tokens + 2 * HALO, tokens + HALO, tokens

    def spid(zz, yy):
        return lax.rem(zz, nz) * ny + lax.rem(yy, ny)

    def rel(j):
        qq, c = j // 2, j % 2
        dx = jnp.where(qq == 0, 0, jnp.where(qq == 1, nx - 1, jnp.where(qq == 2, 1, 2)))
        return lax.rem(x + dx, nx) * 2 + lax.rem(core + c, 2)

    peers = [lax.rem(me + j, tp) for j in range(1, tp)]
    nxt, prv = lax.rem(sp + 1, sp_n), lax.rem(sp + sp_n - 1, sp_n)

    barrier = pltpu.get_barrier_semaphore()

    def greet(dev):
        pl.semaphore_signal(barrier, inc=1, device_id=dev, device_id_type=MESH)

    for j in range(1, ny):
        greet((spid(z, y + j), me))
    for j in range(1, nz):
        greet((spid(z + j, y), me))
    greet((nxt, me))
    greet((prv, me))
    for p in peers:
        greet((sp, p))

    local = [pltpu.make_async_copy(stream, xb0.at[me, pl.ds(HALO, tokens)], loc.at[0])]
    n = 1
    for l in range(2):
        for h in range(2):
            src = pl.ds(128 * h, 128)
            local.append(pltpu.make_async_copy(
                a_w.at[l, :, src], wag.at[l, z, y, :, pl.ds(256 * h, 128)], loc.at[n]))
            local.append(pltpu.make_async_copy(
                g_w.at[l, :, src], wag.at[l, z, y, :, pl.ds(256 * h + 128, 128)], loc.at[n + 1]))
            n += 2
        local.append(pltpu.make_async_copy(o_w.at[l], wo.at[l, z, y], loc.at[n]))
        n += 1
    for c in local:
        c.start()
    lno[...] = jnp.zeros_like(lno)
    lno[0:2, :] = ln_gain[...]
    lno[2:4, :] = ln_shift[...]
    lnb[me] = lno[...]
    for c in local:
        c.wait()
    pl.semaphore_wait(barrier, ny + nz + tp - 1)

    def weight(stage, path):
        buf, cols = (wag, 256) if stage % 2 == 0 else (wo, 128)
        return buf.at[stage // 2], pl.ds(cols * path, cols)

    def first_send(stage):
        for path in range(2):
            ref, cols = weight(stage, path)
            mine = ref.at[z, y, :, cols]
            for j in range(1, ny if path == 0 else nz):
                to = spid(z, y + j) if path == 0 else spid(z + j, y)
                remote(mine, mine, p1_s.at[path, stage], p1_r.at[path, stage], (to, me)).start()

    def first_all(stage, path):
        ref, cols = weight(stage, path)
        if path == 0:
            return ref.at[0, pl.ds(0, ny - 1), :, cols]
        return ref.at[pl.ds(0, nz - 1), 0, :, cols]

    def first_wait(stage):
        for path in range(2):
            whole = first_all(stage, path)
            remote(whole, whole, p1_s.at[path, stage], p1_r.at[path, stage], (sp, sib)).wait_recv()

    def ring_block(item, path, origin):
        stage, h = ITEMS[item]
        ref, cols = weight(stage, path)
        if path == 0:
            m = ny // SUB[stage]
            return ref.at[origin, pl.ds(h * m, m), :, cols]
        m = nz // SUB[stage]
        return ref.at[pl.ds(h * m, m), origin, :, cols]

    def ring_hops(item, path, way):
        size = nz if path == 0 else ny
        return size // 2 if (item + way) % 2 == 0 else size - 1 - size // 2

    def ring_copy(item, path, way, hop, origin):
        step = 1 if way == 0 else -1
        if path == 0:
            to = spid(z + nz + step, y)
        else:
            to = spid(z, y + ny + step)
        block = ring_block(item, path, origin)
        return remote(block, block, rg_s.at[path, way, item], rg_r.at[path, way, item, hop], (to, me))

    def ring(stage, hop):
        for item, (of, _) in enumerate(ITEMS):
            if of != stage:
                continue
            for path in range(2):
                size, at = (nz, z) if path == 0 else (ny, y)
                for way in range(2):
                    hops = ring_hops(item, path, way)
                    step = 1 if way == 0 else -1
                    origin = lax.rem(at + 2 * size - step * hop, size)
                    if 0 < hop <= hops:
                        ring_copy(item, path, way, hop - 1, origin).wait_recv()
                    if hop < hops:
                        ring_copy(item, path, way, hop, origin).start()

    def ring_drain():
        for item, (stage, _) in enumerate(ITEMS):
            for path in range(2):
                ref, cols = weight(stage, path)
                for way in range(2):
                    hops = ring_hops(item, path, way)
                    if hops == 0:
                        continue
                    if path == 0:
                        whole = ref.at[pl.ds(0, hops), pl.ds(0, ny // SUB[stage]), :, cols]
                    else:
                        whole = ref.at[pl.ds(0, nz // SUB[stage]), pl.ds(0, hops), :, cols]
                    remote(whole, whole, rg_s.at[path, way, item], rg_s.at[path, way, item], (sp, sib)).wait_send()
        for stage in range(4):
            for path in range(2):
                whole = first_all(stage, path)
                remote(whole, whole, p1_s.at[path, stage], p1_r.at[path, stage], (sp, sib)).wait_send()

    def x_hops(half, way):
        return nx // 2 if (half + way) % 2 == 0 else nx - 1 - nx // 2

    def x_order(way):
        return (0, 1) if way == 0 else (1, 0)

    def x_piece(buf, rows, half, owner):
        cut = (rows // 2 + BLK - 1) // BLK * BLK
        return buf.at[owner, pl.ds(0, cut) if half == 0 else pl.ds(cut, rows - cut)]

    def x_owner(way, hop):
        step = 1 if way == 0 else -1
        return lax.rem(x + 2 * nx - step * hop, nx) * 2 + core

    def x_copy(g, buf, rows, half, way, hop):
        step = 1 if way == 0 else -1
        to = lax.rem(x + nx + step, nx) * 2 + core
        piece = x_piece(buf, rows, half, x_owner(way, hop))
        return remote(piece, piece, xg_s.at[g, way, half, hop], xg_r.at[g, way, half, hop], (sp, to))

    def d_copy(g, buf, rows, half, way, hop):
        piece = x_piece(buf, rows, half, x_owner(way, hop))
        return remote(piece, piece, dd_s.at[g, way, half, hop - 1], dd_r.at[g, way, half, hop - 1], (sp, sib))

    def own_copy(g, buf, rows):
        piece = buf.at[me, pl.ds(0, rows)]
        return remote(piece, piece, do_s.at[g], do_r.at[g], (sp, sib))

    def x_pieces(hop):
        return [(half, way) for k in range(2) for way in range(2)
                for half in (x_order(way)[k],) if hop <= x_hops(half, way)]

    def gather_start(g, buf, rows):
        for half, way in x_pieces(1):
            x_copy(g, buf, rows, half, way, 0).start()
        own_copy(g, buf, rows).start()

    def gather_hop(g, buf, rows, hop):
        for half, way in x_pieces(hop):
            x_copy(g, buf, rows, half, way, hop - 1).wait_recv()
            if hop < x_hops(half, way):
                x_copy(g, buf, rows, half, way, hop).start()
            d_copy(g, buf, rows, half, way, hop).start()

    def gather_pair(g, buf, rows, hop):
        for half, way in x_pieces(hop):
            d_copy(g, buf, rows, half, way, hop).wait_recv()

    def gather_drain(g, buf, rows):
        own_copy(g, buf, rows).wait_send()
        for hop in range(1, nx // 2 + 1):
            for half, way in x_pieces(hop):
                x_copy(g, buf, rows, half, way, hop - 1).wait_send()
                d_copy(g, buf, rows, half, way, hop).wait_send()

    def blocks(rows, body):
        def run(b, carry):
            body(pl.multiple_of(b * BLK, BLK))
            return carry
        lax.fori_loop(0, rows // BLK, run, 0)

    def wide(ref, l, p):
        return ref[l, p].reshape(C, ref.shape[-1])

    def matmul(l, ref, rows, lo, hi):
        cols = ref.shape[-1]

        def run(j, carry):
            part = jnp.dot(u[j, 0:rows, :], wide(ref, l, rel(j)), preferred_element_type=jnp.float32)
            acc[0:rows, 0:cols] = acc[0:rows, 0:cols] + part
            return carry
        lax.fori_loop(lo, hi, run, 0)

    def clear(rows):
        def body(i):
            acc[pl.ds(i, BLK), :] = jnp.zeros((BLK, 2 * C), jnp.float32)
        blocks(rows, body)

    def prepare(l, buf, rows, lo, hi):
        def run(j, carry):
            p = rel(j)
            gain = norm_gain[l, p]

            def body(i):
                v = buf[p, pl.ds(i, BLK), :].astype(jnp.float32)
                sq = v * v
                part = sq[:, 0:128] + sq[:, 128:256]
                ss[pl.ds(i, BLK), :] = ss[pl.ds(i, BLK), :] + part
                u[j, pl.ds(i, BLK), :] = (v * gain).astype(jnp.bfloat16)
            blocks(rows, body)
            return carry
        lax.fori_loop(lo, hi, run, 0)

    def clear_squares(rows):
        def body(i):
            ss[pl.ds(i, BLK), :] = jnp.zeros((BLK, 128), jnp.float32)
        blocks(rows, body)

    def gate(rows, margin):
        def body(i):
            total = jnp.sum(ss[pl.ds(i, BLK), :], axis=1, keepdims=True)
            factor = lax.rsqrt(total * (1.0 / d_model) + EPSILON)
            at = sp * tokens - margin + i + lax.broadcasted_iota(jnp.int32, (BLK, 128), 0)
            inside = (at >= 0) & (at < tokens * sp_n)
            for h in range(2):
                lin = acc[pl.ds(i, BLK), 256 * h:256 * h + 128] * factor
                gat = acc[pl.ds(i, BLK), 256 * h + 128:256 * h + 256] * factor
                val = jnp.where(inside, lin * jax.nn.sigmoid(gat), 0.0)
                gs[h, pl.ds(i, BLK), :] = val.astype(jnp.bfloat16).astype(jnp.float32)
        blocks(rows, body)

    def convolve(l, buf, rows):
        lane = lax.broadcasted_iota(jnp.int32, (BLK, 128), 1)

        def body(i):
            sums = []
            for h in range(2):
                cols = slice(128 * h, 128 * h + 128)
                total = jnp.broadcast_to(conv_b[l, :, cols], (BLK, 128))
                for k in range(width):
                    total = total + gs[h, pl.ds(i + (1 + k), BLK), :] * conv_w[l, k:k + 1, cols]
                sums.append(total)
            mean = jnp.sum(sums[0] + sums[1], axis=1, keepdims=True) * (1.0 / C)
            low, high = sums[0] - mean, sums[1] - mean
            spread = jnp.sum(low * low + high * high, axis=1, keepdims=True)
            buf[me, pl.ds(i, BLK), 0:128] = low.astype(jnp.bfloat16)
            buf[me, pl.ds(i, BLK), 128:256] = high.astype(jnp.bfloat16)
            st[pl.ds(i, BLK), :] = jnp.where(lane == 0, mean, jnp.where(lane == 1, spread, 0.0))
        blocks(rows, body)

    def stats_send(l):
        so[l] = st[...].T[0:8, :]
        sb[l, me] = so[l]
        for p in peers:
            remote(so.at[l], sb.at[l, me], st_s.at[l], st_r.at[l], (sp, p)).start()

    def stats_all(l):
        whole = sb.at[l, pl.ds(0, tp - 1)]
        return remote(whole, whole, st_s.at[l], st_r.at[l], (sp, sib))

    def stats_take(l):
        stats_all(l).wait_recv()
        means = [sb[l, rel(j), 0:1, :] for j in range(tp)]
        spreads = [sb[l, rel(j), 1:2, :] for j in range(tp)]
        average = sum(means) * (1.0 / tp)
        apart = [m - average for m in means]
        variance = sum(spreads) * (1.0 / d_model) + sum(v * v for v in apart) * (1.0 / tp)
        q[0:tp, :] = jnp.concatenate(apart, axis=0)
        q[tp:tp + 8, :] = jnp.broadcast_to(lax.rsqrt(variance + EPSILON), (8, q.shape[1]))
        qt[...] = q[...].T

    def mix(l, buf, rows, js):
        for j in js:
            p = rel(j)
            gain = lnb[p, l:l + 1, :]
            shift = lnb[p, 2 + l:3 + l, :]

            def body(i):
                v = buf[p, pl.ds(i, BLK), :].astype(jnp.float32)
                v = (v + qt[pl.ds(i, BLK), j:j + 1]) * qt[pl.ds(i, BLK), tp:tp + 1] * gain + shift
                u[j, pl.ds(i, BLK), :] = (v * jax.nn.sigmoid(v)).astype(jnp.bfloat16)
            blocks(rows, body)

    def finish(src, rows, skip, dst):
        def body(i):
            old = src[me, pl.ds(pl.multiple_of(i + skip, 16), BLK), :].astype(jnp.float32)
            dst[pl.ds(i, BLK), :] = (old + acc[pl.ds(i, BLK), 0:C]).astype(jnp.bfloat16)
        blocks(rows, body)

    near = min(6, tp)

    halo = [
        remote(xb0.at[me, pl.ds(HALO, HALO)], xb0.at[me, pl.ds(HALO + tokens, HALO)],
               hl_s.at[0], hl_r.at[0], (prv, me)),
        remote(xb0.at[me, pl.ds(tokens, HALO)], xb0.at[me, pl.ds(0, HALO)],
               hl_s.at[1], hl_r.at[1], (nxt, me)),
    ]
    for c in halo:
        c.start()
    first_send(0)
    for p in peers:
        remote(lno, lnb.at[me], ln_s.at[0], ln_r.at[0], (sp, p)).start()
    ln_all = remote(lnb.at[pl.ds(0, tp - 1)], lnb.at[pl.ds(0, tp - 1)], ln_s.at[0], ln_r.at[0], (sp, sib))
    clear(r0)
    clear_squares(r0)
    for c in halo:
        c.wait_recv()
    gather_start(0, xb0, r0)
    first_send(1)
    prepare(0, xb0, r0, 0, 1)
    first_wait(0)
    ring(0, 0)
    first_send(2)
    gather_hop(0, xb0, r0, 1)
    first_wait(1)
    ring(1, 0)
    ring(0, 1)
    first_send(3)
    own_copy(0, xb0, r0).wait_recv()
    gather_pair(0, xb0, r0, 1)
    prepare(0, xb0, r0, 1, near)
    ring(0, 2)
    for hop in range(2, nx // 2 + 1):
        gather_hop(0, xb0, r0, hop)
        gather_pair(0, xb0, r0, hop)
    prepare(0, xb0, r0, near, tp)
    ring(0, 3)
    ring(1, 1)
    first_wait(2)
    ring(2, 0)
    ring(0, 4)
    matmul(0, wag, r0, 0, tp)
    ring(1, 2)
    gate(r0, HALO)
    ring(2, 1)
    convolve(0, mb0, r1)
    stats_send(0)
    gather_start(1, mb0, r1)
    ring(1, 3)
    ring(1, 4)
    first_wait(3)
    ring(3, 0)
    ring(2, 2)
    clear(r1)
    ln_all.wait_recv()
    stats_take(0)
    mix(0, mb0, r1, [0])
    gather_hop(1, mb0, r1, 1)
    ring(2, 3)
    own_copy(1, mb0, r1).wait_recv()
    gather_pair(1, mb0, r1, 1)
    mix(0, mb0, r1, range(1, near))
    matmul(0, wo, r1, 0, near)
    for hop in range(2, nx // 2 + 1):
        gather_hop(1, mb0, r1, hop)
        gather_pair(1, mb0, r1, hop)
    mix(0, mb0, r1, range(near, tp))
    matmul(0, wo, r1, near, tp)
    finish(xb0, r1, 16, xb1.at[me])
    gather_start(2, xb1, r1)
    ring(2, 4)
    ring(3, 1)
    clear(r1)
    clear_squares(r1)
    prepare(1, xb1, r1, 0, 1)
    matmul(1, wag, r1, 0, 1)
    ring(3, 2)
    gather_hop(2, xb1, r1, 1)
    ring(3, 3)
    own_copy(2, xb1, r1).wait_recv()
    gather_pair(2, xb1, r1, 1)
    prepare(1, xb1, r1, 1, near)
    matmul(1, wag, r1, 1, near)
    for hop in range(2, nx // 2 + 1):
        gather_hop(2, xb1, r1, hop)
        gather_pair(2, xb1, r1, hop)
    prepare(1, xb1, r1, near, tp)
    matmul(1, wag, r1, near, tp)
    gate(r1, HALO // 2)
    convolve(1, mb1, r2)
    stats_send(1)
    gather_start(3, mb1, r2)
    ring(3, 4)
    clear(r2)
    stats_take(1)
    mix(1, mb1, r2, [0])
    gather_hop(3, mb1, r2, 1)
    own_copy(3, mb1, r2).wait_recv()
    gather_pair(3, mb1, r2, 1)
    mix(1, mb1, r2, range(1, near))
    matmul(1, wo, r2, 0, near)
    for hop in range(2, nx // 2 + 1):
        gather_hop(3, mb1, r2, hop)
        gather_pair(3, mb1, r2, hop)
    mix(1, mb1, r2, range(near, tp))
    matmul(1, wo, r2, near, tp)
    finish(xb1, r2, 16, out)

    ring_drain()
    gather_drain(0, xb0, r0)
    gather_drain(1, mb0, r1)
    gather_drain(2, xb1, r1)
    gather_drain(3, mb1, r2)
    for c in halo:
        c.wait_send()
    stats_all(0).wait_send()
    stats_all(1).wait_send()
    ln_all.wait_send()


def build(mesh, nz, ny, nx):
    tp = 2 * nx
    spec = (
        P("sp", "tp"), P(), P(None, "sp", "tp"), P(None, "sp", "tp"), P(None, None, "tp"),
        P(None, "tp"), P(None, "tp"), P(None, "tp"), P(None, "sp", "tp"),
    )

    def local(stream, norm_gain, a_w, g_w, conv_w, conv_b, ln_gain, ln_shift, o_w):
        tokens = stream.shape[0]
        width = conv_w.shape[1]
        kb = a_w.shape[1]
        r0, r1, r2 = tokens + 2 * HALO, tokens + HALO, tokens
        lanes = (r1 + 127) // 128 * 128
        dma, f32, b16 = pltpu.SemaphoreType.DMA, jnp.float32, jnp.bfloat16
        hops = max(nz, ny) // 2
        anywhere = pl.BlockSpec(memory_space=pl.ANY)
        inside = pl.BlockSpec(memory_space=pltpu.VMEM)
        return pl.pallas_call(
            functools.partial(kernel, nz, ny, nx, tokens, width),
            out_shape=jax.ShapeDtypeStruct((tokens, C), b16),
            in_specs=[anywhere] * 4 + [inside] * 5,
            out_specs=inside,
            scratch_shapes=[
                pltpu.VMEM((2, nz, ny, kb, 2 * C), b16),
                pltpu.VMEM((2, nz, ny, kb, C), b16),
                pltpu.VMEM((tp, r0, C), b16),
                pltpu.VMEM((tp, r1, C), b16),
                pltpu.VMEM((tp, r1, C), b16),
                pltpu.VMEM((tp, r2, C), b16),
                pltpu.VMEM((tp, r0, C), b16),
                pltpu.VMEM((2, r0 + BLK, 128), f32),
                pltpu.VMEM((r0, 2 * C), f32),
                pltpu.VMEM((r0, 128), f32),
                pltpu.VMEM((lanes, 128), f32),
                pltpu.VMEM((2, 8, lanes), f32),
                pltpu.VMEM((2, tp, 8, lanes), f32),
                pltpu.VMEM((128, lanes), f32),
                pltpu.VMEM((lanes, 128), f32),
                pltpu.VMEM((8, C), f32),
                pltpu.VMEM((tp, 8, C), f32),
                dma((2, 4)), dma((2, 4)),
                dma((2, 2, len(ITEMS))), dma((2, 2, len(ITEMS), hops)),
                dma((4, 2, 2, 2)), dma((4, 2, 2, 2)),
                dma((4, 2, 2, 2)), dma((4, 2, 2, 2)),
                dma((4,)), dma((4,)),
                dma((2,)), dma((2,)),
                dma((2,)), dma((2,)),
                dma((1,)), dma((1,)),
                dma((16,)),
            ],
            compiler_params=pltpu.CompilerParams(
                collective_id=0, has_side_effects=True, vmem_limit_bytes=56 * 1024 * 1024
            ),
        )(
            stream, a_w, g_w, o_w, norm_gain.reshape(2, tp, 1, C), conv_w,
            conv_b.reshape(2, 1, C), ln_gain, ln_shift,
        )

    return jax.shard_map(local, mesh=mesh, in_specs=spec, out_specs=P("sp", "tp"), check_vma=False)


def solution(mesh):
    return build(mesh, 8, 8, 4)
```

```python
import functools

import jax
import jax.numpy as jnp
from jax import lax
from jax.experimental import pallas as pl
from jax.experimental.pallas import tpu as pltpu
from jax.sharding import PartitionSpec as P

EPSILON = 1e-06
MESH = pl.DeviceIdType.MESH
C = 256
HALO = 32
BLK = 32
SUB = (4, 2, 4, 2)
ITEMS = [(st, h) for st in range(4) for h in range(SUB[st])]


def remote(src, dst, ssem, rsem, dev):
    return pltpu.make_async_remote_copy(
        src_ref=src, dst_ref=dst, send_sem=ssem, recv_sem=rsem, device_id=dev, device_id_type=MESH
    )


def kernel(
    nz, ny, nx, tokens, width,
    stream, a_w, g_w, o_w, norm_gain, conv_w, conv_b, ln_gain, ln_shift,
    out,
    wag, wo, xb0, xb1, mb0, mb1, u, gs, acc, ss, st, so, sb, q, qt, lno, lnb,
    p1_s, p1_r, rg_s, rg_r, xg_s, xg_r, dd_s, dd_r, do_s, do_r, hl_s, hl_r, st_s, st_r, ln_s, ln_r, loc,
):
    tp = 2 * nx
    sp_n = nz * ny
    d_model = C * tp
    kb = d_model // sp_n
    sp = lax.axis_index("sp")
    me = lax.axis_index("tp")
    z, y = sp // ny, lax.rem(sp, ny)
    x, core = me // 2, lax.rem(me, 2)
    sib = me + 1 - 2 * core
    r0, r1, r2 = tokens + 2 * HALO, tokens + HALO, tokens

    def spid(zz, yy):
        return lax.rem(zz, nz) * ny + lax.rem(yy, ny)

    peers = [lax.rem(me + j, tp) for j in range(1, tp)]
    nxt, prv = lax.rem(sp + 1, sp_n), lax.rem(sp + sp_n - 1, sp_n)

    barrier = pltpu.get_barrier_semaphore()

    def greet(dev):
        pl.semaphore_signal(barrier, inc=1, device_id=dev, device_id_type=MESH)

    for j in range(1, ny):
        greet((spid(z, y + j), me))
    for j in range(1, nz):
        greet((spid(z + j, y), me))
    greet((nxt, me))
    greet((prv, me))
    for p in peers:
        greet((sp, p))

    local = [pltpu.make_async_copy(stream, xb0.at[me, pl.ds(HALO, tokens)], loc.at[0])]
    n = 1
    for l in range(2):
        for h in range(2):
            src = pl.ds(128 * h, 128)
            local.append(pltpu.make_async_copy(
                a_w.at[l, :, src], wag.at[l, z, y, :, pl.ds(256 * h, 128)], loc.at[n]))
            local.append(pltpu.make_async_copy(
                g_w.at[l, :, src], wag.at[l, z, y, :, pl.ds(256 * h + 128, 128)], loc.at[n + 1]))
            n += 2
        local.append(pltpu.make_async_copy(o_w.at[l], wo.at[l, z, y], loc.at[n]))
        n += 1
    for c in local:
        c.start()
    lno[...] = jnp.zeros_like(lno)
    lno[0:2, :] = ln_gain[...]
    lno[2:4, :] = ln_shift[...]
    lnb[me] = lno[...]
    for c in local:
        c.wait()
    pl.semaphore_wait(barrier, ny + nz + tp - 1)

    def weight(stage, path):
        buf, cols = (wag, 256) if stage % 2 == 0 else (wo, 128)
        return buf.at[stage // 2], pl.ds(cols * path, cols)

    def first_send(stage):
        for path in range(2):
            ref, cols = weight(stage, path)
            mine = ref.at[z, y, :, cols]
            for j in range(1, ny if path == 0 else nz):
                to = spid(z, y + j) if path == 0 else spid(z + j, y)
                remote(mine, mine, p1_s.at[path, stage], p1_r.at[path, stage], (to, me)).start()

    def first_all(stage, path):
        ref, cols = weight(stage, path)
        if path == 0:
            return ref.at[0, pl.ds(0, ny - 1), :, cols]
        return ref.at[pl.ds(0, nz - 1), 0, :, cols]

    def first_wait(stage):
        for path in range(2):
            whole = first_all(stage, path)
            remote(whole, whole, p1_s.at[path, stage], p1_r.at[path, stage], (sp, sib)).wait_recv()

    def ring_block(item, path, origin):
        stage, h = ITEMS[item]
        ref, cols = weight(stage, path)
        if path == 0:
            m = ny // SUB[stage]
            return ref.at[origin, pl.ds(h * m, m), :, cols]
        m = nz // SUB[stage]
        return ref.at[pl.ds(h * m, m), origin, :, cols]

    def ring_hops(item, path, way):
        size = nz if path == 0 else ny
        return size // 2 if (item + way) % 2 == 0 else size - 1 - size // 2

    def ring_copy(item, path, way, hop, origin):
        step = 1 if way == 0 else -1
        if path == 0:
            to = spid(z + nz + step, y)
        else:
            to = spid(z, y + ny + step)
        block = ring_block(item, path, origin)
        return remote(block, block, rg_s.at[path, way, item], rg_r.at[path, way, item, hop], (to, me))

    def ring(stage, hop):
        for item, (of, _) in enumerate(ITEMS):
            if of != stage:
                continue
            for path in range(2):
                size, at = (nz, z) if path == 0 else (ny, y)
                for way in range(2):
                    hops = ring_hops(item, path, way)
                    step = 1 if way == 0 else -1
                    origin = lax.rem(at + 2 * size - step * hop, size)
                    if 0 < hop <= hops:
                        ring_copy(item, path, way, hop - 1, origin).wait_recv()
                    if hop < hops:
                        ring_copy(item, path, way, hop, origin).start()

    def ring_drain():
        for item, (stage, _) in enumerate(ITEMS):
            for path in range(2):
                ref, cols = weight(stage, path)
                for way in range(2):
                    hops = ring_hops(item, path, way)
                    if hops == 0:
                        continue
                    if path == 0:
                        whole = ref.at[pl.ds(0, hops), pl.ds(0, ny // SUB[stage]), :, cols]
                    else:
                        whole = ref.at[pl.ds(0, nz // SUB[stage]), pl.ds(0, hops), :, cols]
                    remote(whole, whole, rg_s.at[path, way, item], rg_s.at[path, way, item], (sp, sib)).wait_send()
        for stage in range(4):
            for path in range(2):
                whole = first_all(stage, path)
                remote(whole, whole, p1_s.at[path, stage], p1_r.at[path, stage], (sp, sib)).wait_send()

    def x_hops(half, way):
        return nx // 2 if (half + way) % 2 == 0 else nx - 1 - nx // 2

    def x_order(way):
        return (0, 1) if way == 0 else (1, 0)

    def x_piece(buf, rows, half, owner):
        cut = (rows // 2 + BLK - 1) // BLK * BLK
        return buf.at[owner, pl.ds(0, cut) if half == 0 else pl.ds(cut, rows - cut)]

    def x_owner(way, hop):
        step = 1 if way == 0 else -1
        return lax.rem(x + 2 * nx - step * hop, nx) * 2 + core

    def x_copy(g, buf, rows, half, way, hop):
        step = 1 if way == 0 else -1
        to = lax.rem(x + nx + step, nx) * 2 + core
        piece = x_piece(buf, rows, half, x_owner(way, hop))
        return remote(piece, piece, xg_s.at[g, way, half, hop], xg_r.at[g, way, half, hop], (sp, to))

    def d_copy(g, buf, rows, half, way, hop):
        piece = x_piece(buf, rows, half, x_owner(way, hop))
        return remote(piece, piece, dd_s.at[g, way, half, hop - 1], dd_r.at[g, way, half, hop - 1], (sp, sib))

    def own_copy(g, buf, rows):
        piece = buf.at[me, pl.ds(0, rows)]
        return remote(piece, piece, do_s.at[g], do_r.at[g], (sp, sib))

    def x_pieces(hop):
        return [(half, way) for k in range(2) for way in range(2)
                for half in (x_order(way)[k],) if hop <= x_hops(half, way)]

    def gather_start(g, buf, rows):
        for half, way in x_pieces(1):
            x_copy(g, buf, rows, half, way, 0).start()
        own_copy(g, buf, rows).start()

    def gather_hop(g, buf, rows, hop):
        for half, way in x_pieces(hop):
            x_copy(g, buf, rows, half, way, hop - 1).wait_recv()
            if hop < x_hops(half, way):
                x_copy(g, buf, rows, half, way, hop).start()
            d_copy(g, buf, rows, half, way, hop).start()

    def gather_pair(g, buf, rows, hop):
        for half, way in x_pieces(hop):
            d_copy(g, buf, rows, half, way, hop).wait_recv()

    def gather_drain(g, buf, rows):
        own_copy(g, buf, rows).wait_send()
        for hop in range(1, nx // 2 + 1):
            for half, way in x_pieces(hop):
                x_copy(g, buf, rows, half, way, hop - 1).wait_send()
                d_copy(g, buf, rows, half, way, hop).wait_send()

    def blocks(rows, body):
        for i in range(0, rows, BLK):
            body(i)

    def pair_chip(k):
        return lax.rem(x + (0, nx - 1, 1, 2)[k], nx)

    def each(k, body):
        def run(c, carry):
            body(pair_chip(k) * 2 + c)
            return carry
        lax.fori_loop(0, 2, run, 0)

    def lanes(p):
        return pl.ds(pl.multiple_of(p * C, C), C)

    def matmul(l, ref, rows, ks):
        cols = ref.shape[-1]
        for k in ks:
            chip = pair_chip(k)
            left = u[0:rows, pl.ds(pl.multiple_of(chip * 2 * C, 2 * C), 2 * C)]
            right = ref[l, pl.ds(chip * 2, 2)].reshape(2 * C, cols)
            part = jnp.dot(left, right, preferred_element_type=jnp.float32)
            if k == 0:
                acc[0:rows, 0:cols] = part
            else:
                acc[0:rows, 0:cols] = acc[0:rows, 0:cols] + part

    def matmul_whole(l, ref, rows):
        cols = ref.shape[-1]
        for h in range(cols // C):
            right = ref[l, :, :, :, C * h:C * h + C].reshape(d_model, C)
            acc[0:rows, C * h:C * h + C] = jnp.dot(
                u[0:rows, :], right, preferred_element_type=jnp.float32)

    def prepare(l, buf, rows, k):
        def chunk(p):
            gain = norm_gain[l:l + 1, lanes(p)]

            def body(i):
                v = buf[p, i:i + BLK, :].astype(jnp.float32)
                sq = v * v
                ss[i:i + BLK, :] = ss[i:i + BLK, :] + (sq[:, 0:128] + sq[:, 128:256])
                u[i:i + BLK, lanes(p)] = (v * gain).astype(jnp.bfloat16)
            blocks(rows, body)
        each(k, chunk)

    def clear_squares(rows):
        ss[0:rows, :] = jnp.zeros((rows, 128), jnp.float32)

    def factors(rows):
        def body(i):
            total = jnp.sum(ss[i:i + BLK, :], axis=1, keepdims=True)
            ss[i:i + BLK, :] = jnp.broadcast_to(lax.rsqrt(total * (1.0 / d_model) + EPSILON), (BLK, 128))
        blocks(rows, body)

    def gate(rows, margin):
        first = sp * tokens - margin
        row = lax.broadcasted_iota(jnp.int32, (BLK, 128), 0)

        def body(i):
            factor = ss[i:i + BLK, :]
            at = first + i + row
            inside = (at >= 0) & (at < tokens * sp_n)
            for h in range(2):
                lin = acc[i:i + BLK, 256 * h:256 * h + 128] * factor
                gat = acc[i:i + BLK, 256 * h + 128:256 * h + 256] * factor
                val = lin * (0.5 + 0.5 * jnp.tanh(0.5 * gat))
                val = jnp.where(inside, val, 0.0)
                gs[h, i:i + BLK, :] = val.astype(jnp.bfloat16).astype(jnp.float32)
        blocks(rows, body)

    def convolve(l, buf, rows):
        lane = lax.broadcasted_iota(jnp.int32, (BLK, 128), 1)

        def body(i):
            sums = []
            for h in range(2):
                cols = slice(128 * h, 128 * h + 128)
                total = jnp.broadcast_to(conv_b[l:l + 1, cols], (BLK, 128))
                for k in range(width):
                    total = total + gs[h, i + 1 + k:i + 1 + k + BLK, :] * conv_w[k, l:l + 1, cols]
                sums.append(total)
            mean = jnp.sum(sums[0] + sums[1], axis=1, keepdims=True) * (1.0 / C)
            low, high = sums[0] - mean, sums[1] - mean
            spread = jnp.sum(low * low + high * high, axis=1, keepdims=True)
            buf[me, i:i + BLK, 0:128] = low.astype(jnp.bfloat16)
            buf[me, i:i + BLK, 128:256] = high.astype(jnp.bfloat16)
            st[i:i + BLK, :] = jnp.where(lane == 0, mean, jnp.where(lane == 1, spread, 0.0))
        blocks(rows, body)

    def stats_send(l):
        both = st[...].T[0:2, :]
        so[l] = both
        sb[l, me] = both
        for p in peers:
            remote(so.at[l], sb.at[l, me], st_s.at[l], st_r.at[l], (sp, p)).start()

    def stats_all(l):
        whole = sb.at[l, pl.ds(0, tp - 1)]
        return remote(whole, whole, st_s.at[l], st_r.at[l], (sp, sib))

    def stats_take(l, rows):
        stats_all(l).wait_recv()
        means = [sb[l, p, 0:1, :] for p in range(tp)]
        spreads = [sb[l, p, 1:2, :] for p in range(tp)]
        average = sum(means) * (1.0 / tp)
        apart = [m - average for m in means]
        variance = sum(spreads) * (1.0 / d_model) + sum(v * v for v in apart) * (1.0 / tp)
        scale = lax.rsqrt(variance + EPSILON)
        wide = q.shape[1]
        q[0:8, :] = jnp.broadcast_to(scale, (8, wide))
        for p in range(tp):
            q[8 + 8 * p:16 + 8 * p, :] = jnp.broadcast_to(apart[p] * scale, (8, wide))
        qt[...] = q[...].T
        for i in range(0, rows, BLK):
            ss[i:i + BLK, :] = jnp.broadcast_to(qt[i:i + BLK, 0:1], (BLK, 128))

    def mix(l, buf, rows, k):
        lane = lax.broadcasted_iota(jnp.int32, (BLK, 128), 1)

        def chunk(p):
            gain = lnb[p, l:l + 1, :] * 0.5
            shift = lnb[p, 2 + l:3 + l, :] * 0.5
            pick = lane == 8 + 8 * p

            def body(i):
                moved = jnp.sum(jnp.where(pick, qt[i:i + BLK, :], 0.0), axis=1, keepdims=True)
                scale = ss[i:i + BLK, :]
                for h in range(2):
                    cols = slice(128 * h, 128 * h + 128)
                    v = buf[p, i:i + BLK, cols].astype(jnp.float32)
                    v = (v * scale + moved) * gain[:, cols] + shift[:, cols]
                    at = pl.ds(pl.multiple_of(p * C + 128 * h, 128), 128)
                    u[i:i + BLK, at] = (v + v * jnp.tanh(v)).astype(jnp.bfloat16)
            blocks(rows, body)
        each(k, chunk)

    def finish(src, rows, skip, dst):
        def body(i):
            old = src[me, i + skip:i + skip + BLK, :].astype(jnp.float32)
            dst[i:i + BLK, :] = (old + acc[i:i + BLK, 0:C]).astype(jnp.bfloat16)
        blocks(rows, body)

    near = range(1, min(3, nx))
    far = range(3, nx)
    last = range(2, nx // 2 + 1)

    halo = [
        remote(xb0.at[me, pl.ds(HALO, HALO)], xb0.at[me, pl.ds(HALO + tokens, HALO)],
               hl_s.at[0], hl_r.at[0], (prv, me)),
        remote(xb0.at[me, pl.ds(tokens, HALO)], xb0.at[me, pl.ds(0, HALO)],
               hl_s.at[1], hl_r.at[1], (nxt, me)),
    ]
    for c in halo:
        c.start()
    first_send(0)
    for p in peers:
        remote(lno, lnb.at[me], ln_s.at[0], ln_r.at[0], (sp, p)).start()
    ln_all = remote(lnb.at[pl.ds(0, tp - 1)], lnb.at[pl.ds(0, tp - 1)], ln_s.at[0], ln_r.at[0], (sp, sib))
    clear_squares(r0)
    for c in halo:
        c.wait_recv()
    gather_start(0, xb0, r0)
    first_wait(0)
    ring(0, 0)
    first_send(1)
    own_copy(0, xb0, r0).wait_recv()
    prepare(0, xb0, r0, 0)
    ring(0, 1)
    gather_hop(0, xb0, r0, 1)
    first_wait(1)
    ring(1, 0)
    gather_pair(0, xb0, r0, 1)
    ring(0, 2)
    for k in near:
        prepare(0, xb0, r0, k)
    ring(0, 3)
    for hop in last:
        gather_hop(0, xb0, r0, hop)
        gather_pair(0, xb0, r0, hop)
    for k in far:
        prepare(0, xb0, r0, k)
    factors(r0)
    ring(1, 1)
    first_send(2)
    ring(0, 4)
    matmul_whole(0, wag, r0)
    ring(1, 2)
    gate(r0, HALO)
    first_wait(2)
    ring(2, 0)
    convolve(0, mb0, r1)
    stats_send(0)
    gather_start(1, mb0, r1)
    ring(1, 3)
    first_send(3)
    ring(2, 1)
    ln_all.wait_recv()
    stats_take(0, r1)
    ring(1, 4)
    own_copy(1, mb0, r1).wait_recv()
    mix(0, mb0, r1, 0)
    matmul(0, wo, r1, [0])
    gather_hop(1, mb0, r1, 1)
    ring(2, 2)
    gather_pair(1, mb0, r1, 1)
    for k in near:
        mix(0, mb0, r1, k)
    matmul(0, wo, r1, near)
    first_wait(3)
    ring(3, 0)
    for hop in last:
        gather_hop(1, mb0, r1, hop)
        gather_pair(1, mb0, r1, hop)
    for k in far:
        mix(0, mb0, r1, k)
    matmul(0, wo, r1, far)
    finish(xb0, r1, 16, xb1.at[me])
    gather_start(2, xb1, r1)
    ring(2, 3)
    clear_squares(r1)
    ring(2, 4)
    own_copy(2, xb1, r1).wait_recv()
    prepare(1, xb1, r1, 0)
    matmul(1, wag, r1, [0])
    ring(3, 1)
    gather_hop(2, xb1, r1, 1)
    gather_pair(2, xb1, r1, 1)
    for k in near:
        prepare(1, xb1, r1, k)
    matmul(1, wag, r1, near)
    ring(3, 2)
    for hop in last:
        gather_hop(2, xb1, r1, hop)
        gather_pair(2, xb1, r1, hop)
    for k in far:
        prepare(1, xb1, r1, k)
    matmul(1, wag, r1, far)
    factors(r1)
    gate(r1, HALO // 2)
    ring(3, 3)
    convolve(1, mb1, r2)
    stats_send(1)
    gather_start(3, mb1, r2)
    ring(3, 4)
    stats_take(1, r2)
    own_copy(3, mb1, r2).wait_recv()
    mix(1, mb1, r2, 0)
    matmul(1, wo, r2, [0])
    gather_hop(3, mb1, r2, 1)
    gather_pair(3, mb1, r2, 1)
    for k in near:
        mix(1, mb1, r2, k)
    matmul(1, wo, r2, near)
    for hop in last:
        gather_hop(3, mb1, r2, hop)
        gather_pair(3, mb1, r2, hop)
    for k in far:
        mix(1, mb1, r2, k)
    matmul(1, wo, r2, far)
    finish(xb1, r2, 16, out)

    ring_drain()
    gather_drain(0, xb0, r0)
    gather_drain(1, mb0, r1)
    gather_drain(2, xb1, r1)
    gather_drain(3, mb1, r2)
    for c in halo:
        c.wait_send()
    stats_all(0).wait_send()
    stats_all(1).wait_send()
    ln_all.wait_send()


def build(mesh, nz, ny, nx):
    tp = 2 * nx
    spec = (
        P("sp", "tp"), P(), P(None, "sp", "tp"), P(None, "sp", "tp"), P(None, None, "tp"),
        P(None, "tp"), P(None, "tp"), P(None, "tp"), P(None, "sp", "tp"),
    )

    def local(stream, norm_gain, a_w, g_w, conv_w, conv_b, ln_gain, ln_shift, o_w):
        tokens = stream.shape[0]
        width = conv_w.shape[1]
        kb = a_w.shape[1]
        r0, r1, r2 = tokens + 2 * HALO, tokens + HALO, tokens
        lanes = (r1 + 127) // 128 * 128
        dma, f32, b16 = pltpu.SemaphoreType.DMA, jnp.float32, jnp.bfloat16
        hops = max(nz, ny) // 2
        anywhere = pl.BlockSpec(memory_space=pl.ANY)
        inside = pl.BlockSpec(memory_space=pltpu.VMEM)
        return pl.pallas_call(
            functools.partial(kernel, nz, ny, nx, tokens, width),
            out_shape=jax.ShapeDtypeStruct((tokens, C), b16),
            in_specs=[anywhere] * 4 + [inside] * 5,
            out_specs=inside,
            scratch_shapes=[
                pltpu.VMEM((2, nz, ny, kb, 2 * C), b16),
                pltpu.VMEM((2, nz, ny, kb, C), b16),
                pltpu.VMEM((tp, r0, C), b16),
                pltpu.VMEM((tp, r1, C), b16),
                pltpu.VMEM((tp, r1, C), b16),
                pltpu.VMEM((tp, r2, C), b16),
                pltpu.VMEM((r0, tp * C), b16),
                pltpu.VMEM((2, r0 + BLK, 128), f32),
                pltpu.VMEM((r0, 2 * C), f32),
                pltpu.VMEM((r0, 128), f32),
                pltpu.VMEM((lanes, 128), f32),
                pltpu.VMEM((2, 2, lanes), f32),
                pltpu.VMEM((2, tp, 2, lanes), f32),
                pltpu.VMEM((128, lanes), f32),
                pltpu.VMEM((lanes, 128), f32),
                pltpu.VMEM((8, C), f32),
                pltpu.VMEM((tp, 8, C), f32),
                dma((2, 4)), dma((2, 4)),
                dma((2, 2, len(ITEMS))), dma((2, 2, len(ITEMS), hops)),
                dma((4, 2, 2, 2)), dma((4, 2, 2, 2)),
                dma((4, 2, 2, 2)), dma((4, 2, 2, 2)),
                dma((4,)), dma((4,)),
                dma((2,)), dma((2,)),
                dma((2,)), dma((2,)),
                dma((1,)), dma((1,)),
                dma((16,)),
            ],
            compiler_params=pltpu.CompilerParams(
                collective_id=0, has_side_effects=True, vmem_limit_bytes=56 * 1024 * 1024
            ),
        )(
            stream, a_w, g_w, o_w, norm_gain, jnp.transpose(conv_w, (1, 0, 2)), conv_b, ln_gain, ln_shift,
        )

    return jax.shard_map(local, mesh=mesh, in_specs=spec, out_specs=P("sp", "tp"), check_vma=False)


def solution(mesh):
    return build(mesh, 8, 8, 4)
```

```python
import functools

import jax
import jax.numpy as jnp
from jax import lax
from jax.experimental import pallas as pl
from jax.experimental.pallas import tpu as pltpu
from jax.sharding import PartitionSpec as P

EPSILON = 1e-06
MESH = pl.DeviceIdType.MESH
C = 256
HALO = 32
BLK = 32
SUB = (4, 2, 4, 1)
ITEMS = [(st, h) for st in range(4) for h in range(SUB[st])]


def remote(src, dst, ssem, rsem, dev):
    return pltpu.make_async_remote_copy(
        src_ref=src, dst_ref=dst, send_sem=ssem, recv_sem=rsem, device_id=dev, device_id_type=MESH
    )


def kernel(
    nz, ny, nx, tokens, width,
    stream, a_w, g_w, o_w, norm_gain_in, conv_w_in, conv_b_in, ln_gain_in, ln_shift_in,
    out,
    norm_gain, conv_w, conv_b, ln_gain, ln_shift, outv, wag, wo, xb0, xb1, mb0, mb1, u, gs, acc, ss, sc, st, so, sb, q, qt, lno, lnb,
    p1_s, p1_r, po_r, rg_s, rg_r, xg_s, xg_r, dd_r, do_r, hl_s, hl_r, st_s, st_r, ln_s, ln_r, loc,
):
    tp = 2 * nx
    sp_n = nz * ny
    d_model = C * tp
    kb = d_model // sp_n
    sp = lax.axis_index("sp")
    me = lax.axis_index("tp")
    z, y = sp // ny, lax.rem(sp, ny)
    x, core = me // 2, lax.rem(me, 2)
    sib = me + 1 - 2 * core
    r0, r1, r2 = tokens + 2 * HALO, tokens + HALO, tokens
    cut = (r1 // 2 + BLK - 1) // BLK * BLK

    def spid(zz, yy):
        return lax.rem(zz, nz) * ny + lax.rem(yy, ny)

    peers = [lax.rem(me + j, tp) for j in range(1, tp)]
    nxt, prv = lax.rem(sp + 1, sp_n), lax.rem(sp + sp_n - 1, sp_n)

    barrier = pltpu.get_barrier_semaphore()

    def greet(dev):
        pl.semaphore_signal(barrier, inc=1, device_id=dev, device_id_type=MESH)

    for j in range(1, ny):
        greet((spid(z, y + j), me))
    for j in range(1, nz):
        greet((spid(z + j, y), me))
    greet((nxt, me))
    greet((prv, me))
    for p in peers:
        greet((sp, p))

    local = [pltpu.make_async_copy(stream, xb0.at[me, pl.ds(HALO, tokens)], loc.at[0]),
             pltpu.make_async_copy(o_w, wo.at[:, z, y], loc.at[1])]
    for l in range(2):
        for h in range(2):
            src = pl.ds(128 * h, 128)
            pltpu.make_async_copy(
                a_w.at[l, :, src], wag.at[l, z, y, :, pl.ds(256 * h, 128)], loc.at[2]).start()
            pltpu.make_async_copy(
                g_w.at[l, :, src], wag.at[l, z, y, :, pl.ds(256 * h + 128, 128)], loc.at[2]).start()
    pairs = pltpu.make_async_copy(wag.at[:, z, y], wag.at[:, z, y], loc.at[2])
    n = 3
    small = [pltpu.make_async_copy(src, dst, loc.at[n + i]) for i, (src, dst) in enumerate((
        (ln_gain_in, ln_gain), (ln_shift_in, ln_shift), (norm_gain_in, norm_gain),
        (conv_w_in, conv_w), (conv_b_in, conv_b)))]
    for c in local + small:
        c.start()
    for c in small[0:2]:
        c.wait()
    lno[...] = jnp.zeros_like(lno)
    lno[0:2, :] = ln_gain[...]
    lno[2:4, :] = ln_shift[...]
    lnb[me] = lno[...]
    for c in local + small[2:]:
        c.wait()
    pairs.wait()
    pl.semaphore_wait(barrier, ny + nz + tp - 1)

    def weight(stage, path):
        buf, cols = (wag, 256) if stage % 2 == 0 else (wo, 128)
        return buf.at[stage // 2], pl.ds(cols * path, cols)

    def first_axis(path):
        return (ny, y) if path == 0 else (nz, z)

    def first_to(path, index):
        return (spid(z, index), me) if path == 0 else (spid(index, y), me)

    def first_some(stage, path, count):
        ref, cols = weight(stage, path)
        if path == 0:
            return ref.at[0, pl.ds(0, count), :, cols]
        return ref.at[pl.ds(0, count), 0, :, cols]

    def first_send(stage):
        reach = [0, 0]
        for path in range(2):
            size, at = first_axis(path)
            reach[path] = [j for d in range(1, size // 2 + 1) for j in sorted({d, size - d})]
        for i in range(max(len(r) for r in reach)):
            for path in range(2):
                size, at = first_axis(path)
                if i >= len(reach[path]):
                    continue
                ref, cols = weight(stage, path)
                mine = ref.at[z, y, :, cols]
                to = lax.rem(at + reach[path][i], size)
                part = size // SUB[0]
                slot = lax.rem(at // part - to // part + SUB[0], SUB[0])
                arrived = p1_r.at[path, slot] if stage == 0 else po_r.at[path, stage - 1]
                remote(mine, mine, p1_s.at[stage], arrived, first_to(path, to)).start()

    def first_wait(slot):
        for path in range(2):
            size, _ = first_axis(path)
            count = size // SUB[0] - (1 if slot == 0 else 0)
            if count:
                whole = first_some(0, path, count)
                remote(whole, whole, p1_s.at[0], p1_r.at[path, slot], (sp, sib)).wait_recv()

    def first_rest(stage):
        for path in range(2):
            whole = first_some(stage, path, first_axis(path)[0] - 1)
            remote(whole, whole, p1_s.at[stage], po_r.at[path, stage - 1], (sp, sib)).wait_recv()

    def ring_block(item, path, origin):
        stage, h = ITEMS[item]
        ref, cols = weight(stage, path)
        if stage == 0:
            size, at = first_axis(path)
            h = lax.rem(at // (size // SUB[0]) + h, SUB[0])
        if path == 0:
            m = ny // SUB[stage]
            return ref.at[origin, pl.ds(h * m, m), :, cols]
        m = nz // SUB[stage]
        return ref.at[pl.ds(h * m, m), origin, :, cols]

    def ring_hops(item, path, way):
        size = nz if path == 0 else ny
        return size // 2 if (item + way) % 2 == 0 else size - 1 - size // 2

    def ring_copy(item, path, way, hop, origin, far=1):
        step = far if way == 0 else -far
        if path == 0:
            to = spid(z + nz + step, y)
        else:
            to = spid(z, y + ny + step)
        block = ring_block(item, path, origin)
        base = 0 if way == 0 else ring_hops(item, path, 0)
        return remote(block, block, rg_s.at[ITEMS[item][0] % 2], rg_r.at[path, item, base + hop], (to, me))

    def ring(stage, hop, only=None):
        order = [i for i, (of, _) in enumerate(ITEMS) if of == stage]
        if stage == 0:
            order = [0, 1, 3, 2]
        for item in order if only is None else only:
            for path in range(2):
                size, at = (nz, z) if path == 0 else (ny, y)
                for way in range(2):
                    hops = ring_hops(item, path, way)
                    jump = hops == size // 2 and hops >= 2
                    step = 1 if way == 0 else -1
                    origin = lax.rem(at + 2 * size - step * hop, size)
                    if 0 < hop <= hops:
                        ring_copy(item, path, way, hop - 1, origin).wait_recv()
                    if hop < hops - (1 if jump else 0):
                        ring_copy(item, path, way, hop, origin).start()
                    if jump and hop == hops - 2:
                        ring_copy(item, path, way, hops - 1, origin, 2).start()

    def ring_drain():
        for ref, sem in (
            (wag.at[:, pl.ds(0, nz - 1)], rg_s.at[0]), (wo.at[:, pl.ds(0, nz - 1)], rg_s.at[1]),
            (wag.at[0, 0, pl.ds(0, ny - 1)], p1_s.at[0]), (wo.at[0, 0, pl.ds(0, ny - 1)], p1_s.at[3]),
            (wo.at[0, 0, pl.ds(0, ny - 1)], p1_s.at[1]), (wag.at[0, 0, pl.ds(0, ny - 1)], p1_s.at[2]),
        ):
            remote(ref, ref, sem, sem, (sp, sib)).wait_send()

    def x_hops(half, way):
        return nx // 2 if (half + way) % 2 == 0 else nx - 1 - nx // 2

    def x_order(way):
        return (0, 1) if way == 0 else (1, 0)

    def span(g):
        if g == 0:
            return xb0, 0, r0
        buf = (mb0, xb1, mb1)[(g - 1) // 2]
        top = (cut, cut, cut - HALO)[(g - 1) // 2]
        rows = (r1, r1, r2)[(g - 1) // 2]
        return (buf, 0, top) if g % 2 == 1 else (buf, top, rows - top)

    def x_piece(g, half, owner):
        buf, lo, rows = span(g)
        mid = (rows // 2 + 15) // 16 * 16
        return buf.at[owner, pl.ds(lo, mid) if half == 0 else pl.ds(lo + mid, rows - mid)]

    def x_owner(way, hop):
        step = 1 if way == 0 else -1
        return lax.rem(x + 2 * nx - step * hop, nx) * 2 + core

    def x_pieces(hop):
        return [(half, way) for k in range(2) for way in range(2)
                for half in (x_order(way)[k],) if hop <= x_hops(half, way)]

    def x_index(half, way, hop):
        flat = [(hp, p) for hp in range(1, nx // 2 + 1) for p in x_pieces(hp)]
        return flat.index((hop, (half, way)))

    def x_copy(g, half, way, hop):
        step = 1 if way == 0 else -1
        to = lax.rem(x + nx + step, nx) * 2 + core
        piece = x_piece(g, half, x_owner(way, hop))
        return remote(piece, piece, xg_s.at[g], xg_r.at[g, x_index(half, way, hop + 1)], (sp, to))

    def d_copy(g, half, way, hop):
        piece = x_piece(g, half, x_owner(way, hop))
        return remote(piece, piece, xg_s.at[g], dd_r.at[g, hop - 1], (sp, sib))

    def own_copy(g):
        buf, lo, rows = span(g)
        piece = buf.at[me, pl.ds(lo, rows)]
        return remote(piece, piece, xg_s.at[g], do_r.at[g], (sp, sib))

    def some(pieces, part):
        return pieces if part is None else pieces[2 * part:2 * part + 2]

    def gather_start(g, part=None):
        for half, way in some(x_pieces(1), part):
            x_copy(g, half, way, 0).start()
        if part != 1:
            own_copy(g).start()

    def gather_hop(g, hop, part=None):
        for half, way in some(x_pieces(hop), part):
            x_copy(g, half, way, hop - 1).wait_recv()
            if hop < x_hops(half, way):
                x_copy(g, half, way, hop).start()
            d_copy(g, half, way, hop).start()

    def gather_pair(g, hop):
        buf, lo, rows = span(g)
        whole = buf.at[pl.ds(0, len(x_pieces(hop)) // 2), pl.ds(lo, rows)]
        remote(whole, whole, xg_s.at[g], dd_r.at[g, hop - 1], (sp, sib)).wait_recv()

    def gather_drain(g):
        buf, lo, rows = span(g)
        whole = buf.at[pl.ds(0, tp - 1), pl.ds(lo, rows)]
        remote(whole, whole, xg_s.at[g], do_r.at[g], (sp, sib)).wait_send()

    def blocks(rng, body):
        for i in range(rng[0], rng[0] + rng[1], BLK):
            body(i)

    def pair_chip(k):
        return lax.rem(x + (0, nx - 1, 1, 2)[k], nx)

    def each(k, body):
        def run(c, carry):
            body(pair_chip(k) * 2 + c)
            return carry
        lax.fori_loop(0, 2, run, 0)

    def lanes(p):
        return pl.ds(pl.multiple_of(p * C, C), C)

    def matmul(l, ref, rng, ks):
        cols = ref.shape[-1]
        rows = slice(rng[0], rng[0] + rng[1])
        for k in ks:
            chip = pair_chip(k)
            left = u[rows, pl.ds(pl.multiple_of(chip * 2 * C, 2 * C), 2 * C)]
            right = ref[l, pl.ds(chip * 2, 2)].reshape(2 * C, cols)
            part = jnp.dot(left, right, preferred_element_type=jnp.float32)
            if k == 0:
                acc[rows, 0:cols] = part
            else:
                acc[rows, 0:cols] = acc[rows, 0:cols] + part

    def matmul_whole(l, ref, rng):
        cols = ref.shape[-1]
        rows = slice(rng[0], rng[0] + rng[1])
        for h in range(cols // C):
            right = ref[l, :, :, :, C * h:C * h + C].reshape(d_model, C)
            acc[rows, C * h:C * h + C] = jnp.dot(u[rows, :], right, preferred_element_type=jnp.float32)

    def prepare(l, buf, rng, k):
        def chunk(p):
            gain = norm_gain[l:l + 1, lanes(p)]

            def body(i):
                v = buf[p, i:i + BLK, :].astype(jnp.float32)
                sq = v * v
                ss[i:i + BLK, :] = ss[i:i + BLK, :] + (sq[:, 0:128] + sq[:, 128:256])
                u[i:i + BLK, lanes(p)] = (v * gain).astype(jnp.bfloat16)
            blocks(rng, body)
        each(k, chunk)

    def clear_squares(rng):
        ss[rng[0]:rng[0] + rng[1], :] = jnp.zeros((rng[1], 128), jnp.float32)

    def factors(rng):
        def body(i):
            total = jnp.sum(ss[i:i + BLK, :], axis=1, keepdims=True)
            ss[i:i + BLK, :] = jnp.broadcast_to(lax.rsqrt(total * (1.0 / d_model) + EPSILON), (BLK, 128))
        blocks(rng, body)

    def gate(rng, margin):
        first = sp * tokens - margin
        row = lax.broadcasted_iota(jnp.int32, (BLK, 128), 0)

        def body(i):
            factor = ss[i:i + BLK, :]
            at = first + i + row
            inside = (at >= 0) & (at < tokens * sp_n)
            for h in range(2):
                lin = acc[i:i + BLK, 256 * h:256 * h + 128] * factor
                gat = acc[i:i + BLK, 256 * h + 128:256 * h + 256] * factor
                val = lin * (0.5 + 0.5 * jnp.tanh(0.5 * gat))
                val = jnp.where(inside, val, 0.0)
                gs[h, i:i + BLK, :] = val.astype(jnp.bfloat16).astype(jnp.float32)
        blocks(rng, body)

    def convolve(l, buf, rng):
        lane = lax.broadcasted_iota(jnp.int32, (BLK, 128), 1)

        def body(i):
            sums = []
            for h in range(2):
                cols = slice(128 * h, 128 * h + 128)
                total = jnp.broadcast_to(conv_b[l:l + 1, cols], (BLK, 128))
                for k in range(width):
                    total = total + gs[h, i + 1 + k:i + 1 + k + BLK, :] * conv_w[k, l:l + 1, cols]
                sums.append(total)
            mean = jnp.sum(sums[0] + sums[1], axis=1, keepdims=True) * (1.0 / C)
            low, high = sums[0] - mean, sums[1] - mean
            spread = jnp.sum(low * low + high * high, axis=1, keepdims=True)
            buf[me, i:i + BLK, 0:128] = low.astype(jnp.bfloat16)
            buf[me, i:i + BLK, 128:256] = high.astype(jnp.bfloat16)
            r = i - rng[0]
            st[r:r + BLK, :] = jnp.where(lane == 0, mean, jnp.where(lane == 1, spread, 0.0))
        blocks(rng, body)

    def stats_send(l, h):
        both = st[...].T[0:2, :]
        so[l, h] = both
        sb[l, h, me] = both
        for p in peers:
            remote(so.at[l, h], sb.at[l, h, me], st_s.at[2 * l + h], st_r.at[2 * l + h], (sp, p)).start()

    def stats_all(l, h):
        whole = sb.at[l, h, pl.ds(0, tp - 1)]
        return remote(whole, whole, st_s.at[2 * l + h], st_r.at[2 * l + h], (sp, sib))

    def stats_take(l, h):
        stats_all(l, h).wait_recv()
        means = [sb[l, h, p, 0:1, :] for p in range(tp)]
        spreads = [sb[l, h, p, 1:2, :] for p in range(tp)]
        average = sum(means) * (1.0 / tp)
        apart = [m - average for m in means]
        variance = sum(spreads) * (1.0 / d_model) + sum(v * v for v in apart) * (1.0 / tp)
        scale = lax.rsqrt(variance + EPSILON)
        wide = q.shape[1]
        q[0:8, :] = jnp.broadcast_to(scale, (8, wide))
        for p in range(tp):
            q[8 + 8 * p:16 + 8 * p, :] = jnp.broadcast_to(apart[p] * scale, (8, wide))
        qt[h] = q[...].T
        for i in range(0, wide, BLK):
            sc[h, i:i + BLK, :] = jnp.broadcast_to(qt[h, i:i + BLK, 0:1], (BLK, 128))

    def mix(l, buf, rng, h, k):
        lane = lax.broadcasted_iota(jnp.int32, (BLK, 128), 1)

        def chunk(p):
            gain = lnb[p, l:l + 1, :] * 0.5
            shift = lnb[p, 2 + l:3 + l, :] * 0.5
            pick = lane == 8 + 8 * p

            def body(i):
                r = i - rng[0]
                moved = jnp.sum(jnp.where(pick, qt[h, r:r + BLK, :], 0.0), axis=1, keepdims=True)
                scale = sc[h, r:r + BLK, :]
                for c in range(2):
                    cols = slice(128 * c, 128 * c + 128)
                    v = buf[p, i:i + BLK, cols].astype(jnp.float32)
                    v = (v * scale + moved) * gain[:, cols] + shift[:, cols]
                    at = pl.ds(pl.multiple_of(p * C + 128 * c, 128), 128)
                    u[i:i + BLK, at] = (v + v * jnp.tanh(v)).astype(jnp.bfloat16)
            blocks(rng, body)
        each(k, chunk)

    def finish(src, rng, skip, dst):
        def body(i):
            old = src[me, i + skip:i + skip + BLK, :].astype(jnp.float32)
            dst[i:i + BLK, :] = (old + acc[i:i + BLK, 0:C]).astype(jnp.bfloat16)
        blocks(rng, body)

    near = range(1, min(3, nx))
    far = range(3, nx)
    last = range(2, nx // 2 + 1)

    halo = [
        remote(xb0.at[me, pl.ds(HALO, HALO)], xb0.at[me, pl.ds(HALO + tokens, HALO)],
               hl_s.at[0], hl_r.at[0], (prv, me)),
        remote(xb0.at[me, pl.ds(tokens, HALO)], xb0.at[me, pl.ds(0, HALO)],
               hl_s.at[1], hl_r.at[1], (nxt, me)),
    ]
    for c in halo:
        c.start()
    first_send(0)
    first_send(1)
    for p in peers:
        remote(lno, lnb.at[me], ln_s.at[0], ln_r.at[0], (sp, p)).start()
    ln_all = remote(lnb.at[pl.ds(0, tp - 1)], lnb.at[pl.ds(0, tp - 1)], ln_s.at[0], ln_r.at[0], (sp, sib))
    clear_squares((0, r0))
    first_wait(0)
    ring(0, 0, [0])
    first_wait(1)
    ring(0, 0, [1])
    for c in halo:
        c.wait_recv()
    gather_start(0)
    first_wait(3)
    ring(0, 0, [3])
    first_wait(2)
    ring(0, 0, [2])
    ring(0, 1)
    first_rest(1)
    ring(1, 0)
    gather_hop(0, 1, 0)
    ring(0, 2)
    gather_hop(0, 1, 1)
    own_copy(0).wait_recv()
    prepare(0, xb0, (0, r0), 0)
    for hop in last:
        gather_hop(0, hop)
    gather_pair(0, 1)
    for k in near:
        prepare(0, xb0, (0, r0), k)
    for hop in last:
        gather_pair(0, hop)
    for k in far:
        prepare(0, xb0, (0, r0), k)
    factors((0, r0))
    ring(1, 1)
    first_send(2)
    ring(0, 3)
    ring(0, 4)
    top, low = (0, cut + HALO), (cut + HALO, r0 - cut - HALO)
    matmul_whole(0, wag, top)
    gate(top, HALO)
    convolve(0, mb0, (0, cut))
    stats_send(0, 0)
    gather_start(1)
    matmul_whole(0, wag, low)
    gate(low, HALO)
    convolve(0, mb0, (cut, r1 - cut))
    stats_send(0, 1)
    gather_start(2, 0)
    top, low = (0, cut), (cut, r1 - cut)
    ln_all.wait_recv()
    ring(1, 2)
    first_rest(2)
    ring(2, 0)
    stats_take(0, 0)
    own_copy(1).wait_recv()
    mix(0, mb0, top, 0, 0)
    gather_hop(1, 1, 0)
    gather_start(2, 1)
    gather_hop(1, 1, 1)
    stats_take(0, 1)
    own_copy(2).wait_recv()
    mix(0, mb0, low, 1, 0)
    gather_hop(2, 1, 0)
    gather_pair(1, 1)
    for k in near:
        mix(0, mb0, top, 0, k)
    for hop in last:
        gather_hop(1, hop)
    gather_hop(2, 1, 1)
    ring(2, 1)
    first_send(3)
    for hop in last:
        gather_pair(1, hop)
    for k in far:
        mix(0, mb0, top, 0, k)
    ring(1, 3)
    ring(1, 4)
    matmul_whole(0, wo, top)
    finish(xb0, top, 16, xb1.at[me])
    gather_start(3)
    for hop in last:
        gather_hop(2, hop)
    gather_pair(2, 1)
    for k in near:
        mix(0, mb0, low, 1, k)
    for hop in last:
        gather_pair(2, hop)
    for k in far:
        mix(0, mb0, low, 1, k)
    matmul_whole(0, wo, low)
    finish(xb0, low, 16, xb1.at[me])
    gather_start(4, 0)
    clear_squares((0, r1))
    own_copy(3).wait_recv()
    prepare(1, xb1, top, 0)
    ring(2, 2)
    gather_hop(3, 1, 0)
    gather_start(4, 1)
    gather_hop(3, 1, 1)
    first_rest(3)
    ring(3, 0)
    own_copy(4).wait_recv()
    prepare(1, xb1, low, 0)
    gather_pair(3, 1)
    for k in near:
        prepare(1, xb1, top, k)
    gather_hop(4, 1, 0)
    for hop in last:
        gather_hop(3, hop)
    gather_hop(4, 1, 1)
    for hop in last:
        gather_pair(3, hop)
    for k in far:
        prepare(1, xb1, top, k)
    ring(2, 3)
    ring(2, 4)
    matmul_whole(1, wag, top)
    factors(top)
    gate(top, HALO // 2)
    convolve(1, mb1, (0, cut - HALO))
    stats_send(1, 0)
    gather_start(5)
    ring(3, 1)
    for hop in last:
        gather_hop(4, hop)
    gather_pair(4, 1)
    for k in near:
        prepare(1, xb1, low, k)
    for hop in last:
        gather_pair(4, hop)
    ring(3, 2)
    for k in far:
        prepare(1, xb1, low, k)
    matmul_whole(1, wag, low)
    factors(low)
    gate(low, HALO // 2)
    top, low = (0, cut - HALO), (cut - HALO, r2 - cut + HALO)
    convolve(1, mb1, low)
    stats_send(1, 1)
    gather_start(6, 0)
    stats_take(1, 0)
    own_copy(5).wait_recv()
    mix(1, mb1, top, 0, 0)
    gather_hop(5, 1, 0)
    gather_start(6, 1)
    gather_hop(5, 1, 1)
    stats_take(1, 1)
    own_copy(6).wait_recv()
    mix(1, mb1, low, 1, 0)
    gather_hop(6, 1, 0)
    gather_pair(5, 1)
    for k in near:
        mix(1, mb1, top, 0, k)
    ring(3, 3)
    ring(3, 4)
    matmul(1, wo, top, [0])
    matmul(1, wo, top, near)
    for hop in last:
        gather_hop(5, hop)
    gather_hop(6, 1, 1)
    for hop in last:
        gather_pair(5, hop)
    for k in far:
        mix(1, mb1, top, 0, k)
    matmul(1, wo, top, far)
    finish(xb1, top, 16, outv)
    result = [pltpu.make_async_copy(outv.at[pl.ds(*rng)], out.at[pl.ds(*rng)], loc.at[i])
              for i, rng in enumerate((top, low))]
    result[0].start()
    for hop in last:
        gather_hop(6, hop)
    gather_pair(6, 1)
    for k in near:
        mix(1, mb1, low, 1, k)
    matmul(1, wo, low, [0])
    matmul(1, wo, low, near)
    for hop in last:
        gather_pair(6, hop)
    for k in far:
        mix(1, mb1, low, 1, k)
    matmul(1, wo, low, far)
    finish(xb1, low, 16, outv)
    result[1].start()

    ring_drain()
    for g in range(7):
        gather_drain(g)
    for c in halo:
        c.wait_send()
    for l in range(2):
        for h in range(2):
            stats_all(l, h).wait_send()
    ln_all.wait_send()
    for c in result:
        c.wait()


def build(mesh, nz, ny, nx):
    tp = 2 * nx
    spec = (
        P("sp", "tp"), P(), P(None, "sp", "tp"), P(None, "sp", "tp"), P(None, None, "tp"),
        P(None, "tp"), P(None, "tp"), P(None, "tp"), P(None, "sp", "tp"),
    )

    def local(stream, norm_gain, a_w, g_w, conv_w, conv_b, ln_gain, ln_shift, o_w):
        tokens = stream.shape[0]
        width = conv_w.shape[1]
        kb = a_w.shape[1]
        r0, r1, r2 = tokens + 2 * HALO, tokens + HALO, tokens
        lanes = ((r1 // 2 + BLK - 1) // BLK * BLK + 127) // 128 * 128
        dma, f32, b16 = pltpu.SemaphoreType.DMA, jnp.float32, jnp.bfloat16
        hops = max(nz, ny) // 2
        anywhere = pl.BlockSpec(memory_space=pl.ANY)
        return pl.pallas_call(
            functools.partial(kernel, nz, ny, nx, tokens, width),
            out_shape=jax.ShapeDtypeStruct((tokens, C), b16),
            in_specs=[anywhere] * 9,
            out_specs=anywhere,
            scratch_shapes=[
                pltpu.VMEM((2, tp * C), f32),
                pltpu.VMEM((width, 2, C), f32),
                pltpu.VMEM((2, C), f32),
                pltpu.VMEM((2, C), f32),
                pltpu.VMEM((2, C), f32),
                pltpu.VMEM((tokens, C), b16),
                pltpu.VMEM((2, nz, ny, kb, 2 * C), b16),
                pltpu.VMEM((2, nz, ny, kb, C), b16),
                pltpu.VMEM((tp, r0, C), b16),
                pltpu.VMEM((tp, r1, C), b16),
                pltpu.VMEM((tp, r1, C), b16),
                pltpu.VMEM((tp, r2, C), b16),
                pltpu.VMEM((r0, tp * C), b16),
                pltpu.VMEM((2, r0 + BLK, 128), f32),
                pltpu.VMEM((r0, 2 * C), f32),
                pltpu.VMEM((r0, 128), f32),
                pltpu.VMEM((2, lanes, 128), f32),
                pltpu.VMEM((lanes, 128), f32),
                pltpu.VMEM((2, 2, 2, lanes), f32),
                pltpu.VMEM((2, 2, tp, 2, lanes), f32),
                pltpu.VMEM((128, lanes), f32),
                pltpu.VMEM((2, lanes, 128), f32),
                pltpu.VMEM((8, C), f32),
                pltpu.VMEM((tp, 8, C), f32),
                dma((4,)), dma((2, SUB[0])), dma((2, 3)),
                dma((2,)), dma((2, len(ITEMS), 2 * hops - 1)),
                dma((7,)), dma((7, 3 * (nx // 2))), dma((7, nx // 2)), dma((7,)),
                dma((2,)), dma((2,)),
                dma((4,)), dma((4,)),
                dma((1,)), dma((1,)),
                dma((8,)),
            ],
            compiler_params=pltpu.CompilerParams(
                collective_id=0, has_side_effects=True, vmem_limit_bytes=56 * 1024 * 1024
            ),
        )(
            stream, a_w, g_w, o_w, norm_gain, jnp.transpose(conv_w, (1, 0, 2)), conv_b, ln_gain, ln_shift,
        )

    return jax.shard_map(local, mesh=mesh, in_specs=spec, out_specs=P("sp", "tp"), check_vma=False)


def solution(mesh):
    return build(mesh, 8, 8, 4)
```

```python
import functools

import jax
import jax.numpy as jnp
from jax import lax
from jax.experimental import pallas as pl
from jax.experimental.pallas import tpu as pltpu
from jax.sharding import PartitionSpec as P

EPSILON = 1e-06
MESH = pl.DeviceIdType.MESH
C = 256
HALO = 32
BLK = 32
SUB = (4, 2, 4, 1)
ITEMS = [(st, h) for st in range(4) for h in range(SUB[st])]


def remote(src, dst, ssem, rsem, dev):
    return pltpu.make_async_remote_copy(
        src_ref=src, dst_ref=dst, send_sem=ssem, recv_sem=rsem, device_id=dev, device_id_type=MESH
    )


def kernel(
    nz, ny, nx, tokens, width,
    stream, a_w, g_w, o_w, norm_gain_in, conv_w_in, conv_b_in, ln_gain_in, ln_shift_in,
    out,
    norm_gain, conv_w, conv_b, ln_gain, ln_shift, wag, wo, xb0, xb1, mb0, mb1, u, gs, acc, ss, sc, st, so, sb, q, qt, lno, lnb,
    p1_s, p1_r, po_r, rg_s, rg_r, xg_s, xg_r, dd_r, do_r, hl_s, hl_r, st_s, st_r, ln_s, ln_r, loc,
):
    tp = 2 * nx
    sp_n = nz * ny
    d_model = C * tp
    kb = d_model // sp_n
    sp = lax.axis_index("sp")
    me = lax.axis_index("tp")
    z, y = sp // ny, lax.rem(sp, ny)
    x, core = me // 2, lax.rem(me, 2)
    sib = me + 1 - 2 * core
    r0, r1, r2 = tokens + 2 * HALO, tokens + HALO, tokens
    cut = (r1 // 2 + BLK - 1) // BLK * BLK

    def spid(zz, yy):
        return lax.rem(zz, nz) * ny + lax.rem(yy, ny)

    peers = [lax.rem(me + j, tp) for j in range(1, tp)]
    nxt, prv = lax.rem(sp + 1, sp_n), lax.rem(sp + sp_n - 1, sp_n)

    barrier = pltpu.get_barrier_semaphore()

    def greet(dev):
        pl.semaphore_signal(barrier, inc=1, device_id=dev, device_id_type=MESH)

    for j in range(1, ny):
        greet((spid(z, y + j), me))
    for j in range(1, nz):
        greet((spid(z + j, y), me))
    greet((nxt, me))
    greet((prv, me))
    for p in peers:
        greet((sp, p))

    local = [pltpu.make_async_copy(stream, xb0.at[me, pl.ds(HALO, tokens)], loc.at[0]),
             pltpu.make_async_copy(o_w, wo.at[:, z, y], loc.at[1])]
    for l in range(2):
        for h in range(2):
            src = pl.ds(128 * h, 128)
            pltpu.make_async_copy(
                a_w.at[l, :, src], wag.at[l, z, y, :, pl.ds(256 * h, 128)], loc.at[2]).start()
            pltpu.make_async_copy(
                g_w.at[l, :, src], wag.at[l, z, y, :, pl.ds(256 * h + 128, 128)], loc.at[2]).start()
    pairs = pltpu.make_async_copy(wag.at[:, z, y], wag.at[:, z, y], loc.at[2])
    n = 3
    small = [pltpu.make_async_copy(src, dst, loc.at[n + i]) for i, (src, dst) in enumerate((
        (ln_gain_in, ln_gain), (ln_shift_in, ln_shift), (norm_gain_in, norm_gain),
        (conv_w_in, conv_w), (conv_b_in, conv_b)))]
    for c in local + small:
        c.start()
    for c in small[0:2]:
        c.wait()
    lno[...] = jnp.zeros_like(lno)
    lno[0:2, :] = ln_gain[...]
    lno[2:4, :] = ln_shift[...]
    lnb[me] = lno[...]
    for c in local + small[2:]:
        c.wait()
    pairs.wait()
    pl.semaphore_wait(barrier, ny + nz + tp - 1)

    def weight(stage, path):
        buf, cols = (wag, 256) if stage % 2 == 0 else (wo, 128)
        return buf.at[stage // 2], pl.ds(cols * path, cols)

    def first_axis(path):
        return (ny, y) if path == 0 else (nz, z)

    def first_to(path, index):
        return (spid(z, index), me) if path == 0 else (spid(index, y), me)

    def first_some(stage, path, count):
        ref, cols = weight(stage, path)
        if path == 0:
            return ref.at[0, pl.ds(0, count), :, cols]
        return ref.at[pl.ds(0, count), 0, :, cols]

    def first_send(stage):
        reach = [0, 0]
        for path in range(2):
            size, at = first_axis(path)
            reach[path] = [j for d in range(1, size // 2 + 1) for j in sorted({d, size - d})]
        for i in range(max(len(r) for r in reach)):
            for path in range(2):
                size, at = first_axis(path)
                if i >= len(reach[path]):
                    continue
                ref, cols = weight(stage, path)
                mine = ref.at[z, y, :, cols]
                to = lax.rem(at + reach[path][i], size)
                part = size // SUB[0]
                slot = lax.rem(at // part - to // part + SUB[0], SUB[0])
                arrived = p1_r.at[path, slot] if stage == 0 else po_r.at[path, stage - 1]
                remote(mine, mine, p1_s.at[stage], arrived, first_to(path, to)).start()

    def first_wait(slot):
        for path in range(2):
            size, _ = first_axis(path)
            count = size // SUB[0] - (1 if slot == 0 else 0)
            if count:
                whole = first_some(0, path, count)
                remote(whole, whole, p1_s.at[0], p1_r.at[path, slot], (sp, sib)).wait_recv()

    def first_rest(stage):
        for path in range(2):
            whole = first_some(stage, path, first_axis(path)[0] - 1)
            remote(whole, whole, p1_s.at[stage], po_r.at[path, stage - 1], (sp, sib)).wait_recv()

    def ring_block(item, path, origin):
        stage, h = ITEMS[item]
        ref, cols = weight(stage, path)
        if stage == 0:
            size, at = first_axis(path)
            h = lax.rem(at // (size // SUB[0]) + h, SUB[0])
        if path == 0:
            m = ny // SUB[stage]
            return ref.at[origin, pl.ds(h * m, m), :, cols]
        m = nz // SUB[stage]
        return ref.at[pl.ds(h * m, m), origin, :, cols]

    def ring_hops(item, path, way):
        size = nz if path == 0 else ny
        return size // 2 if (item + way) % 2 == 0 else size - 1 - size // 2

    def ring_copy(item, path, way, hop, origin, far=1):
        step = far if way == 0 else -far
        if path == 0:
            to = spid(z + nz + step, y)
        else:
            to = spid(z, y + ny + step)
        block = ring_block(item, path, origin)
        base = 0 if way == 0 else ring_hops(item, path, 0)
        return remote(block, block, rg_s.at[ITEMS[item][0] % 2], rg_r.at[path, item, base + hop], (to, me))

    def ring(stage, hop, only=None):
        order = [i for i, (of, _) in enumerate(ITEMS) if of == stage]
        if stage == 0:
            order = [0, 1, 3, 2]
        for item in order if only is None else only:
            for path in range(2):
                size, at = (nz, z) if path == 0 else (ny, y)
                for way in range(2):
                    hops = ring_hops(item, path, way)
                    jump = hops == size // 2 and hops >= 2
                    step = 1 if way == 0 else -1
                    origin = lax.rem(at + 2 * size - step * hop, size)
                    if 0 < hop <= hops:
                        ring_copy(item, path, way, hop - 1, origin).wait_recv()
                    if hop < hops - (1 if jump else 0):
                        ring_copy(item, path, way, hop, origin).start()
                    if jump and hop == hops - 2:
                        ring_copy(item, path, way, hops - 1, origin, 2).start()

    def ring_drain():
        for ref, sem in (
            (wag.at[:, pl.ds(0, nz - 1)], rg_s.at[0]), (wo.at[:, pl.ds(0, nz - 1)], rg_s.at[1]),
            (wag.at[0, 0, pl.ds(0, ny - 1)], p1_s.at[0]), (wo.at[0, 0, pl.ds(0, ny - 1)], p1_s.at[3]),
            (wo.at[0, 0, pl.ds(0, ny - 1)], p1_s.at[1]), (wag.at[0, 0, pl.ds(0, ny - 1)], p1_s.at[2]),
        ):
            remote(ref, ref, sem, sem, (sp, sib)).wait_send()

    def x_hops(half, way):
        return nx // 2 if (half + way) % 2 == 0 else nx - 1 - nx // 2

    def x_order(way):
        return (0, 1) if way == 0 else (1, 0)

    def span(g):
        if g == 0:
            return xb0, 0, r0
        buf = (mb0, xb1, mb1)[(g - 1) // 2]
        top = (cut, cut, cut - HALO)[(g - 1) // 2]
        rows = (r1, r1, r2)[(g - 1) // 2]
        return (buf, 0, top) if g % 2 == 1 else (buf, top, rows - top)

    def x_piece(g, half, owner):
        buf, lo, rows = span(g)
        mid = (rows // 2 + 15) // 16 * 16
        return buf.at[owner, pl.ds(lo, mid) if half == 0 else pl.ds(lo + mid, rows - mid)]

    def x_owner(way, hop):
        step = 1 if way == 0 else -1
        return lax.rem(x + 2 * nx - step * hop, nx) * 2 + core

    def x_pieces(hop):
        return [(half, way) for k in range(2) for way in range(2)
                for half in (x_order(way)[k],) if hop <= x_hops(half, way)]

    def x_index(half, way, hop):
        flat = [(hp, p) for hp in range(1, nx // 2 + 1) for p in x_pieces(hp)]
        return flat.index((hop, (half, way)))

    def x_copy(g, half, way, hop):
        step = 1 if way == 0 else -1
        to = lax.rem(x + nx + step, nx) * 2 + core
        piece = x_piece(g, half, x_owner(way, hop))
        return remote(piece, piece, xg_s.at[g], xg_r.at[g, x_index(half, way, hop + 1)], (sp, to))

    def d_copy(g, half, way, hop):
        piece = x_piece(g, half, x_owner(way, hop))
        return remote(piece, piece, xg_s.at[g], dd_r.at[g, hop - 1], (sp, sib))

    def own_copy(g):
        buf, lo, rows = span(g)
        piece = buf.at[me, pl.ds(lo, rows)]
        return remote(piece, piece, xg_s.at[g], do_r.at[g], (sp, sib))

    def some(pieces, part):
        return pieces if part is None else pieces[2 * part:2 * part + 2]

    def gather_start(g, part=None):
        for half, way in some(x_pieces(1), part):
            x_copy(g, half, way, 0).start()
        if part != 1:
            own_copy(g).start()

    def gather_hop(g, hop, part=None):
        for half, way in some(x_pieces(hop), part):
            x_copy(g, half, way, hop - 1).wait_recv()
            if hop < x_hops(half, way):
                x_copy(g, half, way, hop).start()
            d_copy(g, half, way, hop).start()

    def gather_pair(g, hop):
        buf, lo, rows = span(g)
        whole = buf.at[pl.ds(0, len(x_pieces(hop)) // 2), pl.ds(lo, rows)]
        remote(whole, whole, xg_s.at[g], dd_r.at[g, hop - 1], (sp, sib)).wait_recv()

    def gather_drain(g):
        buf, lo, rows = span(g)
        whole = buf.at[pl.ds(0, tp - 1), pl.ds(lo, rows)]
        remote(whole, whole, xg_s.at[g], do_r.at[g], (sp, sib)).wait_send()

    def blocks(rng, body):
        for i in range(rng[0], rng[0] + rng[1], BLK):
            body(i)

    def pair_chip(k):
        return lax.rem(x + (0, nx - 1, 1, 2)[k], nx)

    def each(k, body):
        def run(c, carry):
            body(pair_chip(k) * 2 + c)
            return carry
        lax.fori_loop(0, 2, run, 0)

    def lanes(p):
        return pl.ds(pl.multiple_of(p * C, C), C)

    def matmul(l, ref, rng, ks):
        cols = ref.shape[-1]
        rows = slice(rng[0], rng[0] + rng[1])
        for k in ks:
            chip = pair_chip(k)
            left = u[rows, pl.ds(pl.multiple_of(chip * 2 * C, 2 * C), 2 * C)]
            right = ref[l, pl.ds(chip * 2, 2)].reshape(2 * C, cols)
            part = jnp.dot(left, right, preferred_element_type=jnp.float32)
            if k == 0:
                acc[rows, 0:cols] = part
            else:
                acc[rows, 0:cols] = acc[rows, 0:cols] + part

    def matmul_whole(l, ref, rng):
        cols = ref.shape[-1]
        rows = slice(rng[0], rng[0] + rng[1])
        for h in range(cols // C):
            right = ref[l, :, :, :, C * h:C * h + C].reshape(d_model, C)
            acc[rows, C * h:C * h + C] = jnp.dot(u[rows, :], right, preferred_element_type=jnp.float32)

    def prepare(l, buf, rng, k):
        def chunk(p):
            gain = norm_gain[l:l + 1, lanes(p)]

            def body(i):
                v = buf[p, i:i + BLK, :].astype(jnp.float32)
                sq = v * v
                ss[i:i + BLK, :] = ss[i:i + BLK, :] + (sq[:, 0:128] + sq[:, 128:256])
                u[i:i + BLK, lanes(p)] = (v * gain).astype(jnp.bfloat16)
            blocks(rng, body)
        each(k, chunk)

    def clear_squares(rng):
        ss[rng[0]:rng[0] + rng[1], :] = jnp.zeros((rng[1], 128), jnp.float32)

    def factors(rng):
        def body(i):
            total = jnp.sum(ss[i:i + BLK, :], axis=1, keepdims=True)
            ss[i:i + BLK, :] = jnp.broadcast_to(lax.rsqrt(total * (1.0 / d_model) + EPSILON), (BLK, 128))
        blocks(rng, body)

    def gate(rng, margin):
        first = sp * tokens - margin
        row = lax.broadcasted_iota(jnp.int32, (BLK, 128), 0)

        def body(i):
            factor = ss[i:i + BLK, :]
            at = first + i + row
            inside = (at >= 0) & (at < tokens * sp_n)
            for h in range(2):
                lin = acc[i:i + BLK, 256 * h:256 * h + 128] * factor
                gat = acc[i:i + BLK, 256 * h + 128:256 * h + 256] * factor
                val = lin * (0.5 + 0.5 * jnp.tanh(0.5 * gat))
                val = jnp.where(inside, val, 0.0)
                gs[h, i:i + BLK, :] = val.astype(jnp.bfloat16).astype(jnp.float32)
        blocks(rng, body)

    def convolve(l, buf, rng):
        lane = lax.broadcasted_iota(jnp.int32, (BLK, 128), 1)

        def body(i):
            sums = []
            for h in range(2):
                cols = slice(128 * h, 128 * h + 128)
                total = jnp.broadcast_to(conv_b[l:l + 1, cols], (BLK, 128))
                for k in range(width):
                    total = total + gs[h, i + 1 + k:i + 1 + k + BLK, :] * conv_w[k, l:l + 1, cols]
                sums.append(total)
            mean = jnp.sum(sums[0] + sums[1], axis=1, keepdims=True) * (1.0 / C)
            low, high = sums[0] - mean, sums[1] - mean
            spread = jnp.sum(low * low + high * high, axis=1, keepdims=True)
            buf[me, i:i + BLK, 0:128] = low.astype(jnp.bfloat16)
            buf[me, i:i + BLK, 128:256] = high.astype(jnp.bfloat16)
            r = i - rng[0]
            st[r:r + BLK, :] = jnp.where(lane == 0, mean, jnp.where(lane == 1, spread, 0.0))
        blocks(rng, body)

    def stats_send(l, h):
        both = st[...].T[0:2, :]
        so[l, h] = both
        sb[l, h, me] = both
        for p in peers:
            remote(so.at[l, h], sb.at[l, h, me], st_s.at[2 * l + h], st_r.at[2 * l + h], (sp, p)).start()

    def stats_all(l, h):
        whole = sb.at[l, h, pl.ds(0, tp - 1)]
        return remote(whole, whole, st_s.at[2 * l + h], st_r.at[2 * l + h], (sp, sib))

    def stats_take(l, h):
        stats_all(l, h).wait_recv()
        means = [sb[l, h, p, 0:1, :] for p in range(tp)]
        spreads = [sb[l, h, p, 1:2, :] for p in range(tp)]
        average = sum(means) * (1.0 / tp)
        apart = [m - average for m in means]
        variance = sum(spreads) * (1.0 / d_model) + sum(v * v for v in apart) * (1.0 / tp)
        scale = lax.rsqrt(variance + EPSILON)
        wide = q.shape[1]
        q[0:8, :] = jnp.broadcast_to(scale, (8, wide))
        for p in range(tp):
            q[8 + 8 * p:16 + 8 * p, :] = jnp.broadcast_to(apart[p] * scale, (8, wide))
        qt[h] = q[...].T
        for i in range(0, wide, BLK):
            sc[h, i:i + BLK, :] = jnp.broadcast_to(qt[h, i:i + BLK, 0:1], (BLK, 128))

    def mix(l, buf, rng, h, k):
        lane = lax.broadcasted_iota(jnp.int32, (BLK, 128), 1)

        def chunk(p):
            gain = lnb[p, l:l + 1, :] * 0.5
            shift = lnb[p, 2 + l:3 + l, :] * 0.5
            pick = lane == 8 + 8 * p

            def body(i):
                r = i - rng[0]
                moved = jnp.sum(jnp.where(pick, qt[h, r:r + BLK, :], 0.0), axis=1, keepdims=True)
                scale = sc[h, r:r + BLK, :]
                for c in range(2):
                    cols = slice(128 * c, 128 * c + 128)
                    v = buf[p, i:i + BLK, cols].astype(jnp.float32)
                    v = (v * scale + moved) * gain[:, cols] + shift[:, cols]
                    at = pl.ds(pl.multiple_of(p * C + 128 * c, 128), 128)
                    u[i:i + BLK, at] = (v + v * jnp.tanh(v)).astype(jnp.bfloat16)
            blocks(rng, body)
        each(k, chunk)

    def finish(src, rng, skip, dst):
        def body(i):
            old = src[me, i + skip:i + skip + BLK, :].astype(jnp.float32)
            dst[i:i + BLK, :] = (old + acc[i:i + BLK, 0:C]).astype(jnp.bfloat16)
        blocks(rng, body)

    near = range(1, min(3, nx))
    far = range(3, nx)
    last = range(2, nx // 2 + 1)

    halo = [
        remote(xb0.at[me, pl.ds(HALO, HALO)], xb0.at[me, pl.ds(HALO + tokens, HALO)],
               hl_s.at[0], hl_r.at[0], (prv, me)),
        remote(xb0.at[me, pl.ds(tokens, HALO)], xb0.at[me, pl.ds(0, HALO)],
               hl_s.at[1], hl_r.at[1], (nxt, me)),
    ]
    for c in halo:
        c.start()
    first_send(0)
    first_send(1)
    for p in peers:
        remote(lno, lnb.at[me], ln_s.at[0], ln_r.at[0], (sp, p)).start()
    ln_all = remote(lnb.at[pl.ds(0, tp - 1)], lnb.at[pl.ds(0, tp - 1)], ln_s.at[0], ln_r.at[0], (sp, sib))
    clear_squares((0, r0))
    first_wait(0)
    ring(0, 0, [0])
    first_wait(1)
    ring(0, 0, [1])
    for c in halo:
        c.wait_recv()
    gather_start(0)
    first_wait(3)
    ring(0, 0, [3])
    first_wait(2)
    ring(0, 0, [2])
    ring(0, 1)
    first_rest(1)
    ring(1, 0)
    gather_hop(0, 1, 0)
    ring(0, 2)
    gather_hop(0, 1, 1)
    own_copy(0).wait_recv()
    prepare(0, xb0, (0, r0), 0)
    for hop in last:
        gather_hop(0, hop)
    gather_pair(0, 1)
    for k in near:
        prepare(0, xb0, (0, r0), k)
    for hop in last:
        gather_pair(0, hop)
    for k in far:
        prepare(0, xb0, (0, r0), k)
    factors((0, r0))
    ring(1, 1)
    first_send(2)
    ring(0, 3)
    ring(0, 4)
    top, low = (0, cut + HALO), (cut + HALO, r0 - cut - HALO)
    matmul_whole(0, wag, top)
    gate(top, HALO)
    convolve(0, mb0, (0, cut))
    stats_send(0, 0)
    gather_start(1)
    matmul_whole(0, wag, low)
    gate(low, HALO)
    convolve(0, mb0, (cut, r1 - cut))
    stats_send(0, 1)
    gather_start(2, 0)
    top, low = (0, cut), (cut, r1 - cut)
    ln_all.wait_recv()
    ring(1, 2)

    def pass_on():
        gather_hop(1, 1, 0)
        gather_start(2, 1)

    pl.when(core == 1)(pass_on)
    first_rest(2)
    ring(2, 0)
    stats_take(0, 0)
    first_send(3)
    own_copy(1).wait_recv()
    mix(0, mb0, top, 0, 0)
    pl.when(core == 0)(pass_on)
    gather_hop(1, 1, 1)
    stats_take(0, 1)
    own_copy(2).wait_recv()
    mix(0, mb0, low, 1, 0)
    gather_hop(2, 1, 0)
    gather_pair(1, 1)
    for k in near:
        mix(0, mb0, top, 0, k)
    for hop in last:
        gather_hop(1, hop)
    gather_hop(2, 1, 1)
    ring(2, 1)
    for hop in last:
        gather_pair(1, hop)
    for k in far:
        mix(0, mb0, top, 0, k)
    ring(1, 3)
    ring(1, 4)
    matmul_whole(0, wo, top)
    finish(xb0, top, 16, xb1.at[me])
    gather_start(3)
    for hop in last:
        gather_hop(2, hop)
    gather_pair(2, 1)
    for k in near:
        mix(0, mb0, low, 1, k)
    first_rest(3)
    ring(3, 0)
    for hop in last:
        gather_pair(2, hop)
    for k in far:
        mix(0, mb0, low, 1, k)
    matmul_whole(0, wo, low)
    finish(xb0, low, 16, xb1.at[me])
    gather_start(4, 0)
    clear_squares((0, r1))
    own_copy(3).wait_recv()
    prepare(1, xb1, top, 0)
    ring(2, 2)
    gather_hop(3, 1, 0)
    gather_start(4, 1)
    gather_hop(3, 1, 1)
    ring(3, 1)
    own_copy(4).wait_recv()
    prepare(1, xb1, low, 0)
    gather_pair(3, 1)
    for k in near:
        prepare(1, xb1, top, k)
    gather_hop(4, 1, 0)
    for hop in last:
        gather_hop(3, hop)
    gather_hop(4, 1, 1)
    for hop in last:
        gather_pair(3, hop)
    for k in far:
        prepare(1, xb1, top, k)
    ring(2, 3)
    ring(2, 4)
    matmul_whole(1, wag, top)
    factors(top)
    gate(top, HALO // 2)
    convolve(1, mb1, (0, cut - HALO))
    stats_send(1, 0)
    gather_start(5)
    ring(3, 2)
    for hop in last:
        gather_hop(4, hop)
    gather_pair(4, 1)
    for k in near:
        prepare(1, xb1, low, k)
    for hop in last:
        gather_pair(4, hop)
    for k in far:
        prepare(1, xb1, low, k)
    matmul_whole(1, wag, low)
    factors(low)
    gate(low, HALO // 2)
    top, low = (0, cut - HALO), (cut - HALO, r2 - cut + HALO)
    convolve(1, mb1, low)
    stats_send(1, 1)
    gather_start(6, 0)
    stats_take(1, 0)
    own_copy(5).wait_recv()
    mix(1, mb1, top, 0, 0)
    gather_hop(5, 1, 0)
    gather_start(6, 1)
    gather_hop(5, 1, 1)
    stats_take(1, 1)
    own_copy(6).wait_recv()
    mix(1, mb1, low, 1, 0)
    gather_hop(6, 1, 0)
    gather_pair(5, 1)
    for k in near:
        mix(1, mb1, top, 0, k)
    ring(3, 3)
    ring(3, 4)
    matmul(1, wo, top, [0])
    matmul(1, wo, top, near)
    for hop in last:
        gather_hop(5, hop)
    gather_hop(6, 1, 1)
    for hop in last:
        gather_pair(5, hop)
    for k in far:
        mix(1, mb1, top, 0, k)
    matmul(1, wo, top, far)
    finish(xb1, top, 16, out)
    for hop in last:
        gather_hop(6, hop)
    gather_pair(6, 1)
    for k in near:
        mix(1, mb1, low, 1, k)
    matmul(1, wo, low, [0])
    matmul(1, wo, low, near)
    for hop in last:
        gather_pair(6, hop)
    for k in far:
        mix(1, mb1, low, 1, k)
    matmul(1, wo, low, far)
    finish(xb1, low, 16, out)

    ring_drain()
    for g in range(7):
        gather_drain(g)
    for c in halo:
        c.wait_send()
    for l in range(2):
        for h in range(2):
            stats_all(l, h).wait_send()
    ln_all.wait_send()


def build(mesh, nz, ny, nx):
    tp = 2 * nx
    spec = (
        P("sp", "tp"), P(), P(None, "sp", "tp"), P(None, "sp", "tp"), P(None, None, "tp"),
        P(None, "tp"), P(None, "tp"), P(None, "tp"), P(None, "sp", "tp"),
    )

    def local(stream, norm_gain, a_w, g_w, conv_w, conv_b, ln_gain, ln_shift, o_w):
        tokens = stream.shape[0]
        width = conv_w.shape[1]
        kb = a_w.shape[1]
        r0, r1, r2 = tokens + 2 * HALO, tokens + HALO, tokens
        lanes = ((r1 // 2 + BLK - 1) // BLK * BLK + 127) // 128 * 128
        dma, f32, b16 = pltpu.SemaphoreType.DMA, jnp.float32, jnp.bfloat16
        hops = max(nz, ny) // 2
        outside = pl.BlockSpec(memory_space=pltpu.HBM)
        return pl.pallas_call(
            functools.partial(kernel, nz, ny, nx, tokens, width),
            out_shape=jax.ShapeDtypeStruct((tokens, C), b16),
            in_specs=[outside] * 9,
            out_specs=pl.BlockSpec(memory_space=pltpu.VMEM),
            scratch_shapes=[
                pltpu.VMEM((2, tp * C), f32),
                pltpu.VMEM((width, 2, C), f32),
                pltpu.VMEM((2, C), f32),
                pltpu.VMEM((2, C), f32),
                pltpu.VMEM((2, C), f32),
                pltpu.VMEM((2, nz, ny, kb, 2 * C), b16),
                pltpu.VMEM((2, nz, ny, kb, C), b16),
                pltpu.VMEM((tp, r0, C), b16),
                pltpu.VMEM((tp, r1, C), b16),
                pltpu.VMEM((tp, r1, C), b16),
                pltpu.VMEM((tp, r2, C), b16),
                pltpu.VMEM((r0, tp * C), b16),
                pltpu.VMEM((2, r0 + BLK, 128), f32),
                pltpu.VMEM((r0, 2 * C), f32),
                pltpu.VMEM((r0, 128), f32),
                pltpu.VMEM((2, lanes, 128), f32),
                pltpu.VMEM((lanes, 128), f32),
                pltpu.VMEM((2, 2, 2, lanes), f32),
                pltpu.VMEM((2, 2, tp, 2, lanes), f32),
                pltpu.VMEM((128, lanes), f32),
                pltpu.VMEM((2, lanes, 128), f32),
                pltpu.VMEM((8, C), f32),
                pltpu.VMEM((tp, 8, C), f32),
                dma((4,)), dma((2, SUB[0])), dma((2, 3)),
                dma((2,)), dma((2, len(ITEMS), 2 * hops - 1)),
                dma((7,)), dma((7, 3 * (nx // 2))), dma((7, nx // 2)), dma((7,)),
                dma((2,)), dma((2,)),
                dma((4,)), dma((4,)),
                dma((1,)), dma((1,)),
                dma((8,)),
            ],
            compiler_params=pltpu.CompilerParams(
                collective_id=0, has_side_effects=True, vmem_limit_bytes=28 * 1024 * 1024
            ),
        )(
            *[pltpu.with_memory_space_constraint(v, pltpu.HBM) for v in (
            stream, a_w, g_w, o_w, norm_gain, jnp.transpose(conv_w, (1, 0, 2)), conv_b, ln_gain, ln_shift,
            )]
        )

    return jax.shard_map(local, mesh=mesh, in_specs=spec, out_specs=P("sp", "tp"), check_vma=False)


def solution(mesh):
    return build(mesh, 8, 8, 4)
```

```python
import functools

import jax
import jax.numpy as jnp
from jax import lax
from jax.experimental import pallas as pl
from jax.experimental.pallas import tpu as pltpu
from jax.sharding import PartitionSpec as P

EPSILON = 1e-06
MESH = pl.DeviceIdType.MESH
C = 256
HALO = 32
BLK = 32
SUB = (4, 2, 2, 1)
ITEMS = [(st, h) for st in range(4) for h in range(SUB[st])]


def remote(src, dst, ssem, rsem, dev):
    return pltpu.make_async_remote_copy(
        src_ref=src, dst_ref=dst, send_sem=ssem, recv_sem=rsem, device_id=dev, device_id_type=MESH
    )


def kernel(
    nz, ny, nx, tokens, width,
    stream, a_w, g_w, o_w, norm_gain_in, conv_w_in, conv_b_in, ln_gain_in, ln_shift_in,
    out,
    norm_gain, conv_w, conv_b, ln_gain, ln_shift, wag, wo, xb0, xb1, mb0, mb1, u, gs, acc, ss, sc, st, so, sb, q, qt, lno, lnb,
    p1_s, p1_r, po_r, rg_s, rg_r, xg_s, xg_r, dd_r, do_r, hl_s, hl_r, st_s, st_r, ln_s, ln_r, loc,
):
    tp = 2 * nx
    sp_n = nz * ny
    d_model = C * tp
    kb = d_model // sp_n
    sp = lax.axis_index("sp")
    me = lax.axis_index("tp")
    z, y = sp // ny, lax.rem(sp, ny)
    x, core = me // 2, lax.rem(me, 2)
    sib = me + 1 - 2 * core
    r0, r1, r2 = tokens + 2 * HALO, tokens + HALO, tokens
    cut = (r1 // 2 + BLK - 1) // BLK * BLK

    def spid(zz, yy):
        return lax.rem(zz, nz) * ny + lax.rem(yy, ny)

    peers = [lax.rem(me + j, tp) for j in range(1, tp)]
    nxt, prv = lax.rem(sp + 1, sp_n), lax.rem(sp + sp_n - 1, sp_n)

    barrier = pltpu.get_barrier_semaphore()

    def greet(dev):
        pl.semaphore_signal(barrier, inc=1, device_id=dev, device_id_type=MESH)

    for j in range(1, ny):
        greet((spid(z, y + j), me))
    for j in range(1, nz):
        greet((spid(z + j, y), me))
    greet((nxt, me))
    greet((prv, me))
    for p in peers:
        greet((sp, p))

    local = [pltpu.make_async_copy(stream, xb0.at[me, pl.ds(HALO, tokens)], loc.at[0]),
             pltpu.make_async_copy(o_w, wo.at[:, z, y], loc.at[1])]
    for l in range(2):
        for h in range(2):
            src = pl.ds(128 * h, 128)
            pltpu.make_async_copy(
                a_w.at[l, :, src], wag.at[l, z, y, :, pl.ds(256 * h, 128)], loc.at[2]).start()
            pltpu.make_async_copy(
                g_w.at[l, :, src], wag.at[l, z, y, :, pl.ds(256 * h + 128, 128)], loc.at[2]).start()
    pairs = pltpu.make_async_copy(wag.at[:, z, y], wag.at[:, z, y], loc.at[2])
    n = 3
    small = [pltpu.make_async_copy(src, dst, loc.at[n + i]) for i, (src, dst) in enumerate((
        (ln_gain_in, ln_gain), (ln_shift_in, ln_shift), (norm_gain_in, norm_gain),
        (conv_w_in, conv_w), (conv_b_in, conv_b)))]
    for c in local + small:
        c.start()
    for c in small[0:2]:
        c.wait()
    lno[...] = jnp.zeros_like(lno)
    lno[0:2, :] = ln_gain[...]
    lno[2:4, :] = ln_shift[...]
    lnb[me] = lno[...]
    for c in local + small[2:]:
        c.wait()
    pairs.wait()
    pl.semaphore_wait(barrier, ny + nz + tp - 1)

    def weight(stage, path):
        buf, cols = (wag, 256) if stage % 2 == 0 else (wo, 128)
        return buf.at[stage // 2], pl.ds(cols * path, cols)

    def first_axis(path):
        return (ny, y) if path == 0 else (nz, z)

    def first_to(path, index):
        return (spid(z, index), me) if path == 0 else (spid(index, y), me)

    def first_some(stage, path, count):
        ref, cols = weight(stage, path)
        if path == 0:
            return ref.at[0, pl.ds(0, count), :, cols]
        return ref.at[pl.ds(0, count), 0, :, cols]

    def first_send(stage):
        reach = [0, 0]
        for path in range(2):
            size, at = first_axis(path)
            reach[path] = [j for d in range(1, size // 2 + 1) for j in sorted({d, size - d})]
        for i in range(max(len(r) for r in reach)):
            for path in range(2):
                size, at = first_axis(path)
                if i >= len(reach[path]):
                    continue
                ref, cols = weight(stage, path)
                mine = ref.at[z, y, :, cols]
                to = lax.rem(at + reach[path][i], size)
                part = size // SUB[0]
                slot = lax.rem(at // part - to // part + SUB[0], SUB[0])
                arrived = p1_r.at[path, slot] if stage == 0 else po_r.at[path, stage - 1]
                remote(mine, mine, p1_s.at[stage], arrived, first_to(path, to)).start()

    def first_wait(slot):
        for path in range(2):
            size, _ = first_axis(path)
            count = size // SUB[0] - (1 if slot == 0 else 0)
            if count:
                whole = first_some(0, path, count)
                remote(whole, whole, p1_s.at[0], p1_r.at[path, slot], (sp, sib)).wait_recv()

    def first_rest(stage):
        for path in range(2):
            whole = first_some(stage, path, first_axis(path)[0] - 1)
            remote(whole, whole, p1_s.at[stage], po_r.at[path, stage - 1], (sp, sib)).wait_recv()

    def ring_block(item, path, origin):
        stage, h = ITEMS[item]
        ref, cols = weight(stage, path)
        if stage == 0:
            size, at = first_axis(path)
            h = lax.rem(at // (size // SUB[0]) + h, SUB[0])
        if path == 0:
            m = ny // SUB[stage]
            return ref.at[origin, pl.ds(h * m, m), :, cols]
        m = nz // SUB[stage]
        return ref.at[pl.ds(h * m, m), origin, :, cols]

    def ring_hops(item, path, way):
        size = nz if path == 0 else ny
        return size // 2 if (item + way) % 2 == 0 else size - 1 - size // 2

    def ring_copy(item, path, way, hop, origin, far=1):
        step = far if way == 0 else -far
        if path == 0:
            to = spid(z + nz + step, y)
        else:
            to = spid(z, y + ny + step)
        block = ring_block(item, path, origin)
        base = 0 if way == 0 else ring_hops(item, path, 0)
        return remote(block, block, rg_s.at[ITEMS[item][0] % 2], rg_r.at[path, item, base + hop], (to, me))

    def ring(stage, hop, only=None):
        order = [i for i, (of, _) in enumerate(ITEMS) if of == stage]
        if stage == 0:
            order = [0, 1, 3, 2]
        for item in order if only is None else only:
            for path in range(2):
                size, at = (nz, z) if path == 0 else (ny, y)
                for way in range(2):
                    hops = ring_hops(item, path, way)
                    jump = hops == size // 2 and hops >= 2
                    step = 1 if way == 0 else -1
                    origin = lax.rem(at + 2 * size - step * hop, size)
                    if 0 < hop <= hops:
                        ring_copy(item, path, way, hop - 1, origin).wait_recv()
                    if hop < hops - (1 if jump else 0):
                        ring_copy(item, path, way, hop, origin).start()
                    if jump and hop == hops - 2:
                        ring_copy(item, path, way, hops - 1, origin, 2).start()

    def ring_drain():
        for ref, sem in (
            (wag.at[:, pl.ds(0, nz - 1)], rg_s.at[0]), (wo.at[:, pl.ds(0, nz - 1)], rg_s.at[1]),
            (wag.at[0, 0, pl.ds(0, ny - 1)], p1_s.at[0]), (wo.at[0, 0, pl.ds(0, ny - 1)], p1_s.at[3]),
            (wo.at[0, 0, pl.ds(0, ny - 1)], p1_s.at[1]), (wag.at[0, 0, pl.ds(0, ny - 1)], p1_s.at[2]),
        ):
            remote(ref, ref, sem, sem, (sp, sib)).wait_send()

    def x_hops(half, way):
        return nx // 2 if (half + way) % 2 == 0 else nx - 1 - nx // 2

    def x_order(way):
        return (0, 1) if way == 0 else (1, 0)

    def span(g):
        if g == 0:
            return xb0, 0, r0
        buf = (mb0, xb1, mb1)[(g - 1) // 2]
        top = (cut, cut, cut - HALO)[(g - 1) // 2]
        rows = (r1, r1, r2)[(g - 1) // 2]
        return (buf, 0, top) if g % 2 == 1 else (buf, top, rows - top)

    def x_piece(g, half, owner):
        buf, lo, rows = span(g)
        mid = (rows // 2 + 15) // 16 * 16
        return buf.at[owner, pl.ds(lo, mid) if half == 0 else pl.ds(lo + mid, rows - mid)]

    def x_owner(way, hop):
        step = 1 if way == 0 else -1
        return lax.rem(x + 2 * nx - step * hop, nx) * 2 + core

    def x_pieces(hop):
        return [(half, way) for k in range(2) for way in range(2)
                for half in (x_order(way)[k],) if hop <= x_hops(half, way)]

    def x_index(half, way, hop):
        flat = [(hp, p) for hp in range(1, nx // 2 + 1) for p in x_pieces(hp)]
        return flat.index((hop, (half, way)))

    def x_copy(g, half, way, hop):
        step = 1 if way == 0 else -1
        to = lax.rem(x + nx + step, nx) * 2 + core
        piece = x_piece(g, half, x_owner(way, hop))
        return remote(piece, piece, xg_s.at[g], xg_r.at[g, x_index(half, way, hop + 1)], (sp, to))

    def d_copy(g, half, way, hop):
        piece = x_piece(g, half, x_owner(way, hop))
        return remote(piece, piece, xg_s.at[g], dd_r.at[g, hop - 1], (sp, sib))

    def own_copy(g):
        buf, lo, rows = span(g)
        piece = buf.at[me, pl.ds(lo, rows)]
        return remote(piece, piece, xg_s.at[g], do_r.at[g], (sp, sib))

    def some(pieces, part):
        return pieces if part is None else pieces[2 * part:2 * part + 2]

    def gather_start(g, part=None):
        for half, way in some(x_pieces(1), part):
            x_copy(g, half, way, 0).start()
        if part != 1:
            own_copy(g).start()

    def gather_hop(g, hop, part=None):
        for half, way in some(x_pieces(hop), part):
            x_copy(g, half, way, hop - 1).wait_recv()
            if hop < x_hops(half, way):
                x_copy(g, half, way, hop).start()
            d_copy(g, half, way, hop).start()

    def gather_pair(g, hop):
        buf, lo, rows = span(g)
        whole = buf.at[pl.ds(0, len(x_pieces(hop)) // 2), pl.ds(lo, rows)]
        remote(whole, whole, xg_s.at[g], dd_r.at[g, hop - 1], (sp, sib)).wait_recv()

    def gather_drain(g):
        buf, lo, rows = span(g)
        whole = buf.at[pl.ds(0, tp - 1), pl.ds(lo, rows)]
        remote(whole, whole, xg_s.at[g], do_r.at[g], (sp, sib)).wait_send()

    def blocks(rng, body):
        for i in range(rng[0], rng[0] + rng[1], BLK):
            body(i)

    def pair_chip(k):
        return lax.rem(x + (0, nx - 1, 1, 2)[k], nx)

    def each(k, body):
        def run(c, carry):
            body(pair_chip(k) * 2 + c)
            return carry
        lax.fori_loop(0, 2, run, 0)

    def lanes(p):
        return pl.ds(pl.multiple_of(p * C, C), C)

    def matmul(l, ref, rng, ks):
        cols = ref.shape[-1]
        rows = slice(rng[0], rng[0] + rng[1])
        for k in ks:
            chip = pair_chip(k)
            left = u[rows, pl.ds(pl.multiple_of(chip * 2 * C, 2 * C), 2 * C)]
            right = ref[l, pl.ds(chip * 2, 2)].reshape(2 * C, cols)
            part = jnp.dot(left, right, preferred_element_type=jnp.float32)
            if k == 0:
                acc[rows, 0:cols] = part
            else:
                acc[rows, 0:cols] = acc[rows, 0:cols] + part

    def matmul_whole(l, ref, rng):
        cols = ref.shape[-1]
        rows = slice(rng[0], rng[0] + rng[1])
        for h in range(cols // C):
            right = ref[l, :, :, :, C * h:C * h + C].reshape(d_model, C)
            acc[rows, C * h:C * h + C] = jnp.dot(u[rows, :], right, preferred_element_type=jnp.float32)

    def prepare(l, buf, rng, k):
        def chunk(p):
            gain = norm_gain[l:l + 1, lanes(p)]

            def body(i):
                v = buf[p, i:i + BLK, :].astype(jnp.float32)
                sq = v * v
                ss[i:i + BLK, :] = ss[i:i + BLK, :] + (sq[:, 0:128] + sq[:, 128:256])
                u[i:i + BLK, lanes(p)] = (v * gain).astype(jnp.bfloat16)
            blocks(rng, body)
        each(k, chunk)

    def clear_squares(rng):
        ss[rng[0]:rng[0] + rng[1], :] = jnp.zeros((rng[1], 128), jnp.float32)

    def factors(rng):
        def body(i):
            total = jnp.sum(ss[i:i + BLK, :], axis=1, keepdims=True)
            ss[i:i + BLK, :] = jnp.broadcast_to(lax.rsqrt(total * (1.0 / d_model) + EPSILON), (BLK, 128))
        blocks(rng, body)

    def gate(rng, margin):
        first = sp * tokens - margin
        row = lax.broadcasted_iota(jnp.int32, (BLK, 128), 0)

        def body(i):
            factor = ss[i:i + BLK, :]
            at = first + i + row
            inside = (at >= 0) & (at < tokens * sp_n)
            for h in range(2):
                lin = acc[i:i + BLK, 256 * h:256 * h + 128] * factor
                gat = acc[i:i + BLK, 256 * h + 128:256 * h + 256] * factor
                val = lin * (0.5 + 0.5 * jnp.tanh(0.5 * gat))
                val = jnp.where(inside, val, 0.0)
                gs[h, i:i + BLK, :] = val.astype(jnp.bfloat16).astype(jnp.float32)
        blocks(rng, body)

    def convolve(l, buf, rng):
        lane = lax.broadcasted_iota(jnp.int32, (BLK, 128), 1)

        def body(i):
            sums = []
            for h in range(2):
                cols = slice(128 * h, 128 * h + 128)
                total = jnp.broadcast_to(conv_b[l:l + 1, cols], (BLK, 128))
                for k in range(width):
                    total = total + gs[h, i + 1 + k:i + 1 + k + BLK, :] * conv_w[k, l:l + 1, cols]
                sums.append(total)
            mean = jnp.sum(sums[0] + sums[1], axis=1, keepdims=True) * (1.0 / C)
            low, high = sums[0] - mean, sums[1] - mean
            spread = jnp.sum(low * low + high * high, axis=1, keepdims=True)
            buf[me, i:i + BLK, 0:128] = low.astype(jnp.bfloat16)
            buf[me, i:i + BLK, 128:256] = high.astype(jnp.bfloat16)
            r = i - rng[0]
            st[r:r + BLK, :] = jnp.where(lane == 0, mean, jnp.where(lane == 1, spread, 0.0))
        blocks(rng, body)

    def stats_send(l, h):
        both = st[...].T[0:2, :]
        so[l, h] = both
        sb[l, h, me] = both
        for p in peers:
            remote(so.at[l, h], sb.at[l, h, me], st_s.at[2 * l + h], st_r.at[2 * l + h], (sp, p)).start()

    def stats_all(l, h):
        whole = sb.at[l, h, pl.ds(0, tp - 1)]
        return remote(whole, whole, st_s.at[2 * l + h], st_r.at[2 * l + h], (sp, sib))

    def stats_take(l, h):
        stats_all(l, h).wait_recv()
        means = [sb[l, h, p, 0:1, :] for p in range(tp)]
        spreads = [sb[l, h, p, 1:2, :] for p in range(tp)]
        average = sum(means) * (1.0 / tp)
        apart = [m - average for m in means]
        variance = sum(spreads) * (1.0 / d_model) + sum(v * v for v in apart) * (1.0 / tp)
        scale = lax.rsqrt(variance + EPSILON)
        wide = q.shape[1]
        q[0:8, :] = jnp.broadcast_to(scale, (8, wide))
        for p in range(tp):
            q[8 + 8 * p:16 + 8 * p, :] = jnp.broadcast_to(apart[p] * scale, (8, wide))
        qt[h] = q[...].T
        for i in range(0, wide, BLK):
            sc[h, i:i + BLK, :] = jnp.broadcast_to(qt[h, i:i + BLK, 0:1], (BLK, 128))

    def mix(l, buf, rng, h, k):
        lane = lax.broadcasted_iota(jnp.int32, (BLK, 128), 1)

        def chunk(p):
            gain = lnb[p, l:l + 1, :] * 0.5
            shift = lnb[p, 2 + l:3 + l, :] * 0.5
            pick = lane == 8 + 8 * p

            def body(i):
                r = i - rng[0]
                moved = jnp.sum(jnp.where(pick, qt[h, r:r + BLK, :], 0.0), axis=1, keepdims=True)
                scale = sc[h, r:r + BLK, :]
                for c in range(2):
                    cols = slice(128 * c, 128 * c + 128)
                    v = buf[p, i:i + BLK, cols].astype(jnp.float32)
                    v = (v * scale + moved) * gain[:, cols] + shift[:, cols]
                    at = pl.ds(pl.multiple_of(p * C + 128 * c, 128), 128)
                    u[i:i + BLK, at] = (v + v * jnp.tanh(v)).astype(jnp.bfloat16)
            blocks(rng, body)
        each(k, chunk)

    def finish(src, rng, skip, dst):
        def body(i):
            old = src[me, i + skip:i + skip + BLK, :].astype(jnp.float32)
            dst[i:i + BLK, :] = (old + acc[i:i + BLK, 0:C]).astype(jnp.bfloat16)
        blocks(rng, body)

    near = range(1, min(3, nx))
    far = range(3, nx)
    last = range(2, nx // 2 + 1)

    halo = [
        remote(xb0.at[me, pl.ds(HALO, HALO)], xb0.at[me, pl.ds(HALO + tokens, HALO)],
               hl_s.at[0], hl_r.at[0], (prv, me)),
        remote(xb0.at[me, pl.ds(tokens, HALO)], xb0.at[me, pl.ds(0, HALO)],
               hl_s.at[1], hl_r.at[1], (nxt, me)),
    ]
    for c in halo:
        c.start()
    first_send(0)
    first_send(1)
    for p in peers:
        remote(lno, lnb.at[me], ln_s.at[0], ln_r.at[0], (sp, p)).start()
    ln_all = remote(lnb.at[pl.ds(0, tp - 1)], lnb.at[pl.ds(0, tp - 1)], ln_s.at[0], ln_r.at[0], (sp, sib))
    clear_squares((0, r0))
    first_wait(0)
    ring(0, 0, [0])
    first_wait(1)
    ring(0, 0, [1])
    for c in halo:
        c.wait_recv()
    gather_start(0)
    first_wait(3)
    ring(0, 0, [3])
    first_wait(2)
    ring(0, 0, [2])
    ring(0, 1)
    first_rest(1)
    ring(1, 0)
    gather_hop(0, 1, 0)
    ring(0, 2)
    gather_hop(0, 1, 1)
    own_copy(0).wait_recv()
    prepare(0, xb0, (0, r0), 0)
    for hop in last:
        gather_hop(0, hop)
    gather_pair(0, 1)
    for k in near:
        prepare(0, xb0, (0, r0), k)
    for hop in last:
        gather_pair(0, hop)
    for k in far:
        prepare(0, xb0, (0, r0), k)
    factors((0, r0))
    ring(1, 1)
    first_send(2)
    ring(0, 3)
    ring(0, 4)
    top, low = (0, cut + HALO), (cut + HALO, r0 - cut - HALO)
    matmul_whole(0, wag, top)
    gate(top, HALO)
    convolve(0, mb0, (0, cut))
    stats_send(0, 0)
    gather_start(1)
    matmul_whole(0, wag, low)
    gate(low, HALO)
    convolve(0, mb0, (cut, r1 - cut))
    stats_send(0, 1)
    gather_start(2, 0)
    top, low = (0, cut), (cut, r1 - cut)
    ln_all.wait_recv()
    ring(1, 2)

    def pass_on():
        gather_hop(1, 1, 0)
        gather_start(2, 1)

    pl.when(core == 1)(pass_on)
    first_rest(2)
    ring(2, 0)
    stats_take(0, 0)
    first_send(3)
    own_copy(1).wait_recv()
    mix(0, mb0, top, 0, 0)
    pl.when(core == 0)(pass_on)
    gather_hop(1, 1, 1)
    stats_take(0, 1)
    own_copy(2).wait_recv()
    mix(0, mb0, low, 1, 0)
    gather_hop(2, 1, 0)
    gather_pair(1, 1)
    for k in near:
        mix(0, mb0, top, 0, k)
    for hop in last:
        gather_hop(1, hop)
    gather_hop(2, 1, 1)
    ring(2, 1)
    for hop in last:
        gather_pair(1, hop)
    for k in far:
        mix(0, mb0, top, 0, k)
    ring(1, 3)
    ring(1, 4)
    for hop in last:
        gather_hop(2, hop)
    matmul_whole(0, wo, top)
    finish(xb0, top, 16, xb1.at[me])
    gather_start(3)
    gather_pair(2, 1)
    for k in near:
        mix(0, mb0, low, 1, k)
    first_rest(3)
    ring(3, 0)
    for hop in last:
        gather_pair(2, hop)
    for k in far:
        mix(0, mb0, low, 1, k)
    matmul_whole(0, wo, low)
    finish(xb0, low, 16, xb1.at[me])
    gather_start(4, 0)
    clear_squares((0, r1))
    own_copy(3).wait_recv()
    prepare(1, xb1, top, 0)
    ring(2, 2)
    gather_hop(3, 1, 0)
    gather_start(4, 1)
    gather_hop(3, 1, 1)
    ring(3, 1)
    own_copy(4).wait_recv()
    prepare(1, xb1, low, 0)
    gather_pair(3, 1)
    for k in near:
        prepare(1, xb1, top, k)
    gather_hop(4, 1, 0)
    for hop in last:
        gather_hop(3, hop)
    gather_hop(4, 1, 1)
    for hop in last:
        gather_pair(3, hop)
    for k in far:
        prepare(1, xb1, top, k)
    factors(top)
    for hop in last:
        gather_hop(4, hop)
    gather_pair(4, 1)
    for k in near:
        prepare(1, xb1, low, k)
    ring(2, 3)
    ring(2, 4)
    matmul_whole(1, wag, top)
    gate(top, HALO // 2)
    convolve(1, mb1, (0, cut - HALO))
    stats_send(1, 0)
    gather_start(5)
    ring(3, 2)
    for hop in last:
        gather_pair(4, hop)
    for k in far:
        prepare(1, xb1, low, k)
    matmul_whole(1, wag, low)
    factors(low)
    gate(low, HALO // 2)
    top, low = (0, cut - HALO), (cut - HALO, r2 - cut + HALO)
    convolve(1, mb1, low)
    stats_send(1, 1)
    gather_start(6, 0)
    stats_take(1, 0)
    own_copy(5).wait_recv()
    mix(1, mb1, top, 0, 0)
    gather_hop(5, 1, 0)
    gather_start(6, 1)
    gather_hop(5, 1, 1)
    stats_take(1, 1)
    own_copy(6).wait_recv()
    mix(1, mb1, low, 1, 0)
    gather_hop(6, 1, 0)
    gather_pair(5, 1)
    for k in near:
        mix(1, mb1, top, 0, k)
    ring(3, 3)
    ring(3, 4)
    matmul(1, wo, top, [0])
    matmul(1, wo, top, near)
    for hop in last:
        gather_hop(5, hop)
    gather_hop(6, 1, 1)
    for hop in last:
        gather_pair(5, hop)
    for k in far:
        mix(1, mb1, top, 0, k)
    matmul(1, wo, top, far)
    finish(xb1, top, 16, out)
    for hop in last:
        gather_hop(6, hop)
    gather_pair(6, 1)
    for k in near:
        mix(1, mb1, low, 1, k)
    matmul(1, wo, low, [0])
    matmul(1, wo, low, near)
    for hop in last:
        gather_pair(6, hop)
    for k in far:
        mix(1, mb1, low, 1, k)
    matmul(1, wo, low, far)
    finish(xb1, low, 16, out)

    ring_drain()
    for g in range(7):
        gather_drain(g)
    for c in halo:
        c.wait_send()
    for l in range(2):
        for h in range(2):
            stats_all(l, h).wait_send()
    ln_all.wait_send()


def build(mesh, nz, ny, nx):
    tp = 2 * nx
    spec = (
        P("sp", "tp"), P(), P(None, "sp", "tp"), P(None, "sp", "tp"), P(None, None, "tp"),
        P(None, "tp"), P(None, "tp"), P(None, "tp"), P(None, "sp", "tp"),
    )

    def local(stream, norm_gain, a_w, g_w, conv_w, conv_b, ln_gain, ln_shift, o_w):
        tokens = stream.shape[0]
        width = conv_w.shape[1]
        kb = a_w.shape[1]
        r0, r1, r2 = tokens + 2 * HALO, tokens + HALO, tokens
        lanes = ((r1 // 2 + BLK - 1) // BLK * BLK + 127) // 128 * 128
        dma, f32, b16 = pltpu.SemaphoreType.DMA, jnp.float32, jnp.bfloat16
        hops = max(nz, ny) // 2
        outside = pl.BlockSpec(memory_space=pltpu.HBM)
        return pl.pallas_call(
            functools.partial(kernel, nz, ny, nx, tokens, width),
            out_shape=jax.ShapeDtypeStruct((tokens, C), b16),
            in_specs=[outside] * 9,
            out_specs=pl.BlockSpec(memory_space=pltpu.VMEM),
            scratch_shapes=[
                pltpu.VMEM((2, tp * C), f32),
                pltpu.VMEM((width, 2, C), f32),
                pltpu.VMEM((2, C), f32),
                pltpu.VMEM((2, C), f32),
                pltpu.VMEM((2, C), f32),
                pltpu.VMEM((2, nz, ny, kb, 2 * C), b16),
                pltpu.VMEM((2, nz, ny, kb, C), b16),
                pltpu.VMEM((tp, r0, C), b16),
                pltpu.VMEM((tp, r1, C), b16),
                pltpu.VMEM((tp, r1, C), b16),
                pltpu.VMEM((tp, r2, C), b16),
                pltpu.VMEM((r0, tp * C), b16),
                pltpu.VMEM((2, r0 + BLK, 128), f32),
                pltpu.VMEM((r0, 2 * C), f32),
                pltpu.VMEM((r0, 128), f32),
                pltpu.VMEM((2, lanes, 128), f32),
                pltpu.VMEM((lanes, 128), f32),
                pltpu.VMEM((2, 2, 2, lanes), f32),
                pltpu.VMEM((2, 2, tp, 2, lanes), f32),
                pltpu.VMEM((128, lanes), f32),
                pltpu.VMEM((2, lanes, 128), f32),
                pltpu.VMEM((8, C), f32),
                pltpu.VMEM((tp, 8, C), f32),
                dma((4,)), dma((2, SUB[0])), dma((2, 3)),
                dma((2,)), dma((2, len(ITEMS), 2 * hops - 1)),
                dma((7,)), dma((7, 3 * (nx // 2))), dma((7, nx // 2)), dma((7,)),
                dma((2,)), dma((2,)),
                dma((4,)), dma((4,)),
                dma((1,)), dma((1,)),
                dma((8,)),
            ],
            compiler_params=pltpu.CompilerParams(
                collective_id=0, has_side_effects=True, vmem_limit_bytes=28 * 1024 * 1024
            ),
        )(
            *[pltpu.with_memory_space_constraint(v, pltpu.HBM) for v in (
            stream, a_w, g_w, o_w, norm_gain, jnp.transpose(conv_w, (1, 0, 2)), conv_b, ln_gain, ln_shift,
            )]
        )

    return jax.shard_map(local, mesh=mesh, in_specs=spec, out_specs=P("sp", "tp"), check_vma=False)


def solution(mesh):
    return build(mesh, 8, 8, 4)
```

```python
import functools

import jax
import jax.numpy as jnp
from jax import lax
from jax.experimental import pallas as pl
from jax.experimental.pallas import tpu as pltpu
from jax.sharding import PartitionSpec as P

EPSILON = 1e-06
MESH = pl.DeviceIdType.MESH
C = 256
HALO = 32
BLK = 32
SUB = (4, 1, 2, 1)
ITEMS = [(st, h) for st in range(4) for h in range(SUB[st])]


def remote(src, dst, ssem, rsem, dev):
    return pltpu.make_async_remote_copy(
        src_ref=src, dst_ref=dst, send_sem=ssem, recv_sem=rsem, device_id=dev, device_id_type=MESH
    )


def kernel(
    nz, ny, nx, tokens, width,
    stream, a_w, g_w, o_w, norm_gain_in, conv_w_in, conv_b_in, ln_gain_in, ln_shift_in,
    out,
    norm_gain, conv_w, conv_b, ln_gain, ln_shift, wag, wo, xb0, xb1, mb0, mb1, u, gs, acc, ss, sc, st, so, sb, q, qt, lno, lnb,
    p1_s, p1_r, po_r, rg_s, rg_r, xg_s, xg_r, dd_r, do_r, hl_s, hl_r, st_s, st_r, ln_s, ln_r, loc,
):
    tp = 2 * nx
    sp_n = nz * ny
    d_model = C * tp
    kb = d_model // sp_n
    sp = lax.axis_index("sp")
    me = lax.axis_index("tp")
    z, y = sp // ny, lax.rem(sp, ny)
    x, core = me // 2, lax.rem(me, 2)
    sib = me + 1 - 2 * core
    r0, r1, r2 = tokens + 2 * HALO, tokens + HALO, tokens
    cut = (r1 // 2 + BLK - 1) // BLK * BLK

    def spid(zz, yy):
        return lax.rem(zz, nz) * ny + lax.rem(yy, ny)

    peers = [lax.rem(me + j, tp) for j in range(1, tp)]
    nxt, prv = lax.rem(sp + 1, sp_n), lax.rem(sp + sp_n - 1, sp_n)

    barrier = pltpu.get_barrier_semaphore()

    def greet(dev):
        pl.semaphore_signal(barrier, inc=1, device_id=dev, device_id_type=MESH)

    for j in range(1, ny):
        greet((spid(z, y + j), me))
    for j in range(1, nz):
        greet((spid(z + j, y), me))
    greet((nxt, me))
    greet((prv, me))
    for p in peers:
        greet((sp, p))

    local = [pltpu.make_async_copy(stream, xb0.at[me, pl.ds(HALO, tokens)], loc.at[0]),
             pltpu.make_async_copy(o_w, wo.at[:, z, y], loc.at[1])]
    for l in range(2):
        for h in range(2):
            src = pl.ds(128 * h, 128)
            pltpu.make_async_copy(
                a_w.at[l, :, src], wag.at[l, z, y, :, pl.ds(256 * h, 128)], loc.at[2]).start()
            pltpu.make_async_copy(
                g_w.at[l, :, src], wag.at[l, z, y, :, pl.ds(256 * h + 128, 128)], loc.at[2]).start()
    pairs = pltpu.make_async_copy(wag.at[:, z, y], wag.at[:, z, y], loc.at[2])
    n = 3
    small = [pltpu.make_async_copy(src, dst, loc.at[n + i]) for i, (src, dst) in enumerate((
        (ln_gain_in, ln_gain), (ln_shift_in, ln_shift), (norm_gain_in, norm_gain),
        (conv_w_in, conv_w), (conv_b_in, conv_b)))]
    for c in local + small:
        c.start()
    for c in small[0:2]:
        c.wait()
    lno[...] = jnp.zeros_like(lno)
    lno[0:2, :] = ln_gain[...]
    lno[2:4, :] = ln_shift[...]
    lnb[me] = lno[...]
    for c in local + small[2:]:
        c.wait()
    pairs.wait()
    pl.semaphore_wait(barrier, ny + nz + tp - 1)

    def weight(stage, path):
        buf, cols = (wag, 256) if stage % 2 == 0 else (wo, 128)
        return buf.at[stage // 2], pl.ds(cols * path, cols)

    def first_axis(path):
        return (ny, y) if path == 0 else (nz, z)

    def first_to(path, index):
        return (spid(z, index), me) if path == 0 else (spid(index, y), me)

    def first_some(stage, path, count):
        ref, cols = weight(stage, path)
        if path == 0:
            return ref.at[0, pl.ds(0, count), :, cols]
        return ref.at[pl.ds(0, count), 0, :, cols]

    def first_send(stage):
        reach = [0, 0]
        for path in range(2):
            size, at = first_axis(path)
            reach[path] = [j for d in range(1, size // 2 + 1) for j in sorted({d, size - d})]
        for i in range(max(len(r) for r in reach)):
            for path in range(2):
                size, at = first_axis(path)
                if i >= len(reach[path]):
                    continue
                ref, cols = weight(stage, path)
                mine = ref.at[z, y, :, cols]
                to = lax.rem(at + reach[path][i], size)
                part = size // SUB[0]
                slot = lax.rem(at // part - to // part + SUB[0], SUB[0])
                arrived = p1_r.at[path, slot] if stage == 0 else po_r.at[path, stage - 1]
                remote(mine, mine, p1_s.at[stage], arrived, first_to(path, to)).start()

    def first_wait(slot):
        for path in range(2):
            size, _ = first_axis(path)
            count = size // SUB[0] - (1 if slot == 0 else 0)
            if count:
                whole = first_some(0, path, count)
                remote(whole, whole, p1_s.at[0], p1_r.at[path, slot], (sp, sib)).wait_recv()

    def first_rest(stage):
        for path in range(2):
            whole = first_some(stage, path, first_axis(path)[0] - 1)
            remote(whole, whole, p1_s.at[stage], po_r.at[path, stage - 1], (sp, sib)).wait_recv()

    def ring_block(item, path, origin):
        stage, h = ITEMS[item]
        ref, cols = weight(stage, path)
        if stage == 0:
            size, at = first_axis(path)
            h = lax.rem(at // (size // SUB[0]) + h, SUB[0])
        if path == 0:
            m = ny // SUB[stage]
            return ref.at[origin, pl.ds(h * m, m), :, cols]
        m = nz // SUB[stage]
        return ref.at[pl.ds(h * m, m), origin, :, cols]

    def ring_hops(item, path, way):
        size = nz if path == 0 else ny
        return size // 2 if (item + way) % 2 == 0 else size - 1 - size // 2

    def ring_copy(item, path, way, hop, origin, far=1):
        step = far if way == 0 else -far
        if path == 0:
            to = spid(z + nz + step, y)
        else:
            to = spid(z, y + ny + step)
        block = ring_block(item, path, origin)
        base = 0 if way == 0 else ring_hops(item, path, 0)
        return remote(block, block, rg_s.at[ITEMS[item][0] % 2], rg_r.at[path, item, base + hop], (to, me))

    def ring(stage, hop, only=None):
        order = [i for i, (of, _) in enumerate(ITEMS) if of == stage]
        if stage == 0:
            order = [0, 1, 3, 2]
        for item in order if only is None else only:
            for path in range(2):
                size, at = (nz, z) if path == 0 else (ny, y)
                for way in range(2):
                    hops = ring_hops(item, path, way)
                    jump = hops == size // 2 and hops >= 2
                    step = 1 if way == 0 else -1
                    origin = lax.rem(at + 2 * size - step * hop, size)
                    if 0 < hop <= hops:
                        ring_copy(item, path, way, hop - 1, origin).wait_recv()
                    if hop < hops - (1 if jump else 0):
                        ring_copy(item, path, way, hop, origin).start()
                    if jump and hop == hops - 2:
                        ring_copy(item, path, way, hops - 1, origin, 2).start()

    def ring_drain():
        for ref, sem in (
            (wag.at[:, pl.ds(0, nz - 1)], rg_s.at[0]), (wo.at[:, pl.ds(0, nz - 1)], rg_s.at[1]),
            (wag.at[0, 0, pl.ds(0, ny - 1)], p1_s.at[0]), (wo.at[0, 0, pl.ds(0, ny - 1)], p1_s.at[3]),
            (wo.at[0, 0, pl.ds(0, ny - 1)], p1_s.at[1]), (wag.at[0, 0, pl.ds(0, ny - 1)], p1_s.at[2]),
        ):
            remote(ref, ref, sem, sem, (sp, sib)).wait_send()

    def x_hops(half, way):
        return nx // 2 if (half + way) % 2 == 0 else nx - 1 - nx // 2

    def x_order(way):
        return (0, 1) if way == 0 else (1, 0)

    def span(g):
        if g == 0:
            return xb0, 0, r0
        buf = (mb0, xb1, mb1)[(g - 1) // 2]
        top = (cut, cut, cut - HALO)[(g - 1) // 2]
        rows = (r1, r1, r2)[(g - 1) // 2]
        return (buf, 0, top) if g % 2 == 1 else (buf, top, rows - top)

    def x_piece(g, half, owner):
        buf, lo, rows = span(g)
        mid = (rows // 2 + 15) // 16 * 16
        return buf.at[owner, pl.ds(lo, mid) if half == 0 else pl.ds(lo + mid, rows - mid)]

    def x_owner(way, hop):
        step = 1 if way == 0 else -1
        return lax.rem(x + 2 * nx - step * hop, nx) * 2 + core

    def x_pieces(hop):
        return [(half, way) for k in range(2) for way in range(2)
                for half in (x_order(way)[k],) if hop <= x_hops(half, way)]

    def x_index(half, way, hop):
        flat = [(hp, p) for hp in range(1, nx // 2 + 1) for p in x_pieces(hp)]
        return flat.index((hop, (half, way)))

    def x_copy(g, half, way, hop):
        step = 1 if way == 0 else -1
        to = lax.rem(x + nx + step, nx) * 2 + core
        piece = x_piece(g, half, x_owner(way, hop))
        return remote(piece, piece, xg_s.at[g], xg_r.at[g, x_index(half, way, hop + 1)], (sp, to))

    def d_copy(g, half, way, hop):
        piece = x_piece(g, half, x_owner(way, hop))
        return remote(piece, piece, xg_s.at[g], dd_r.at[g, hop - 1], (sp, sib))

    def own_copy(g):
        buf, lo, rows = span(g)
        piece = buf.at[me, pl.ds(lo, rows)]
        return remote(piece, piece, xg_s.at[g], do_r.at[g], (sp, sib))

    def some(pieces, part):
        return pieces if part is None else pieces[2 * part:2 * part + 2]

    def gather_start(g, part=None):
        for half, way in some(x_pieces(1), part):
            x_copy(g, half, way, 0).start()
        if part != 1:
            own_copy(g).start()

    def gather_hop(g, hop, part=None):
        for half, way in some(x_pieces(hop), part):
            x_copy(g, half, way, hop - 1).wait_recv()
            if hop < x_hops(half, way):
                x_copy(g, half, way, hop).start()
            d_copy(g, half, way, hop).start()

    def gather_pair(g, hop):
        buf, lo, rows = span(g)
        whole = buf.at[pl.ds(0, len(x_pieces(hop)) // 2), pl.ds(lo, rows)]
        remote(whole, whole, xg_s.at[g], dd_r.at[g, hop - 1], (sp, sib)).wait_recv()

    def gather_drain(g):
        buf, lo, rows = span(g)
        whole = buf.at[pl.ds(0, tp - 1), pl.ds(lo, rows)]
        remote(whole, whole, xg_s.at[g], do_r.at[g], (sp, sib)).wait_send()

    def blocks(rng, body):
        for i in range(rng[0], rng[0] + rng[1], BLK):
            body(i)

    def pair_chip(k):
        return lax.rem(x + (0, nx - 1, 1, 2)[k], nx)

    def each(k, body):
        def run(c, carry):
            body(pair_chip(k) * 2 + c)
            return carry
        lax.fori_loop(0, 2, run, 0)

    def lanes(p):
        return pl.ds(pl.multiple_of(p * C, C), C)

    def matmul(l, ref, rng, ks):
        cols = ref.shape[-1]
        rows = slice(rng[0], rng[0] + rng[1])
        for k in ks:
            chip = pair_chip(k)
            left = u[rows, pl.ds(pl.multiple_of(chip * 2 * C, 2 * C), 2 * C)]
            right = ref[l, pl.ds(chip * 2, 2)].reshape(2 * C, cols)
            part = jnp.dot(left, right, preferred_element_type=jnp.float32)
            if k == 0:
                acc[rows, 0:cols] = part
            else:
                acc[rows, 0:cols] = acc[rows, 0:cols] + part

    def matmul_whole(l, ref, rng):
        cols = ref.shape[-1]
        rows = slice(rng[0], rng[0] + rng[1])
        for h in range(cols // C):
            right = ref[l, :, :, :, C * h:C * h + C].reshape(d_model, C)
            acc[rows, C * h:C * h + C] = jnp.dot(u[rows, :], right, preferred_element_type=jnp.float32)

    def prepare(l, buf, rng, k):
        def chunk(p):
            gain = norm_gain[l:l + 1, lanes(p)]

            def body(i):
                v = buf[p, i:i + BLK, :].astype(jnp.float32)
                sq = v * v
                ss[i:i + BLK, :] = ss[i:i + BLK, :] + (sq[:, 0:128] + sq[:, 128:256])
                u[i:i + BLK, lanes(p)] = (v * gain).astype(jnp.bfloat16)
            blocks(rng, body)
        each(k, chunk)

    def clear_squares(rng):
        ss[rng[0]:rng[0] + rng[1], :] = jnp.zeros((rng[1], 128), jnp.float32)

    def factors(rng):
        def body(i):
            total = jnp.sum(ss[i:i + BLK, :], axis=1, keepdims=True)
            ss[i:i + BLK, :] = jnp.broadcast_to(lax.rsqrt(total * (1.0 / d_model) + EPSILON), (BLK, 128))
        blocks(rng, body)

    def gate(rng, margin):
        first = sp * tokens - margin
        row = lax.broadcasted_iota(jnp.int32, (BLK, 128), 0)

        def body(i):
            factor = ss[i:i + BLK, :]
            at = first + i + row
            inside = (at >= 0) & (at < tokens * sp_n)
            for h in range(2):
                lin = acc[i:i + BLK, 256 * h:256 * h + 128] * factor
                gat = acc[i:i + BLK, 256 * h + 128:256 * h + 256] * factor
                val = lin * (0.5 + 0.5 * jnp.tanh(0.5 * gat))
                val = jnp.where(inside, val, 0.0)
                gs[h, i:i + BLK, :] = val.astype(jnp.bfloat16).astype(jnp.float32)
        blocks(rng, body)

    def convolve(l, buf, rng):
        lane = lax.broadcasted_iota(jnp.int32, (BLK, 128), 1)

        def body(i):
            sums = []
            for h in range(2):
                cols = slice(128 * h, 128 * h + 128)
                total = jnp.broadcast_to(conv_b[l:l + 1, cols], (BLK, 128))
                for k in range(width):
                    total = total + gs[h, i + 1 + k:i + 1 + k + BLK, :] * conv_w[k, l:l + 1, cols]
                sums.append(total)
            mean = jnp.sum(sums[0] + sums[1], axis=1, keepdims=True) * (1.0 / C)
            low, high = sums[0] - mean, sums[1] - mean
            spread = jnp.sum(low * low + high * high, axis=1, keepdims=True)
            buf[me, i:i + BLK, 0:128] = low.astype(jnp.bfloat16)
            buf[me, i:i + BLK, 128:256] = high.astype(jnp.bfloat16)
            r = i - rng[0]
            st[r:r + BLK, :] = jnp.where(lane == 0, mean, jnp.where(lane == 1, spread, 0.0))
        blocks(rng, body)

    def stats_send(l, h):
        both = st[...].T[0:2, :]
        so[l, h] = both
        sb[l, h, me] = both
        for p in peers:
            remote(so.at[l, h], sb.at[l, h, me], st_s.at[2 * l + h], st_r.at[2 * l + h], (sp, p)).start()

    def stats_all(l, h):
        whole = sb.at[l, h, pl.ds(0, tp - 1)]
        return remote(whole, whole, st_s.at[2 * l + h], st_r.at[2 * l + h], (sp, sib))

    def stats_take(l, h):
        stats_all(l, h).wait_recv()
        means = [sb[l, h, p, 0:1, :] for p in range(tp)]
        spreads = [sb[l, h, p, 1:2, :] for p in range(tp)]
        average = sum(means) * (1.0 / tp)
        apart = [m - average for m in means]
        variance = sum(spreads) * (1.0 / d_model) + sum(v * v for v in apart) * (1.0 / tp)
        scale = lax.rsqrt(variance + EPSILON)
        wide = q.shape[1]
        q[0:8, :] = jnp.broadcast_to(scale, (8, wide))
        for p in range(tp):
            q[8 + 8 * p:16 + 8 * p, :] = jnp.broadcast_to(apart[p] * scale, (8, wide))
        qt[h] = q[...].T
        for i in range(0, wide, BLK):
            sc[h, i:i + BLK, :] = jnp.broadcast_to(qt[h, i:i + BLK, 0:1], (BLK, 128))

    def mix(l, buf, rng, h, k):
        lane = lax.broadcasted_iota(jnp.int32, (BLK, 128), 1)

        def chunk(p):
            gain = lnb[p, l:l + 1, :] * 0.5
            shift = lnb[p, 2 + l:3 + l, :] * 0.5
            pick = lane == 8 + 8 * p

            def body(i):
                r = i - rng[0]
                moved = jnp.sum(jnp.where(pick, qt[h, r:r + BLK, :], 0.0), axis=1, keepdims=True)
                scale = sc[h, r:r + BLK, :]
                for c in range(2):
                    cols = slice(128 * c, 128 * c + 128)
                    v = buf[p, i:i + BLK, cols].astype(jnp.float32)
                    v = (v * scale + moved) * gain[:, cols] + shift[:, cols]
                    at = pl.ds(pl.multiple_of(p * C + 128 * c, 128), 128)
                    u[i:i + BLK, at] = (v + v * jnp.tanh(v)).astype(jnp.bfloat16)
            blocks(rng, body)
        each(k, chunk)

    def finish(src, rng, skip, dst):
        def body(i):
            old = src[me, i + skip:i + skip + BLK, :].astype(jnp.float32)
            dst[i:i + BLK, :] = (old + acc[i:i + BLK, 0:C]).astype(jnp.bfloat16)
        blocks(rng, body)

    near = range(1, min(3, nx))
    far = range(3, nx)
    last = range(2, nx // 2 + 1)

    halo = [
        remote(xb0.at[me, pl.ds(HALO, HALO)], xb0.at[me, pl.ds(HALO + tokens, HALO)],
               hl_s.at[0], hl_r.at[0], (prv, me)),
        remote(xb0.at[me, pl.ds(tokens, HALO)], xb0.at[me, pl.ds(0, HALO)],
               hl_s.at[1], hl_r.at[1], (nxt, me)),
    ]
    for c in halo:
        c.start()
    first_send(0)
    first_send(1)
    for p in peers:
        remote(lno, lnb.at[me], ln_s.at[0], ln_r.at[0], (sp, p)).start()
    ln_all = remote(lnb.at[pl.ds(0, tp - 1)], lnb.at[pl.ds(0, tp - 1)], ln_s.at[0], ln_r.at[0], (sp, sib))
    clear_squares((0, r0))
    first_wait(0)
    ring(0, 0, [0])
    first_wait(1)
    ring(0, 0, [1])
    for c in halo:
        c.wait_recv()
    gather_start(0)
    first_wait(3)
    ring(0, 0, [3])
    first_wait(2)
    ring(0, 0, [2])
    ring(0, 1)
    first_rest(1)
    ring(1, 0)
    gather_hop(0, 1, 0)
    ring(0, 2)
    gather_hop(0, 1, 1)
    own_copy(0).wait_recv()
    prepare(0, xb0, (0, r0), 0)
    for hop in last:
        gather_hop(0, hop)
    gather_pair(0, 1)
    for k in near:
        prepare(0, xb0, (0, r0), k)
    for hop in last:
        gather_pair(0, hop)
    for k in far:
        prepare(0, xb0, (0, r0), k)
    factors((0, r0))
    ring(1, 1)
    first_send(2)
    ring(0, 3)
    ring(0, 4)
    top, low = (0, cut + HALO), (cut + HALO, r0 - cut - HALO)
    matmul_whole(0, wag, top)
    gate(top, HALO)
    convolve(0, mb0, (0, cut))
    stats_send(0, 0)
    gather_start(1)
    matmul_whole(0, wag, low)
    gate(low, HALO)
    convolve(0, mb0, (cut, r1 - cut))
    stats_send(0, 1)
    gather_start(2, 0)
    top, low = (0, cut), (cut, r1 - cut)
    ln_all.wait_recv()
    ring(1, 2)

    def pass_on():
        gather_hop(1, 1, 0)
        gather_start(2, 1)

    pl.when(core == 1)(pass_on)
    first_rest(2)
    ring(2, 0)
    stats_take(0, 0)
    first_send(3)
    own_copy(1).wait_recv()
    mix(0, mb0, top, 0, 0)
    pl.when(core == 0)(pass_on)
    gather_hop(1, 1, 1)
    stats_take(0, 1)
    own_copy(2).wait_recv()
    mix(0, mb0, low, 1, 0)
    gather_hop(2, 1, 0)
    gather_pair(1, 1)
    for k in near:
        mix(0, mb0, top, 0, k)
    for hop in last:
        gather_hop(1, hop)
    gather_hop(2, 1, 1)
    ring(2, 1)
    for hop in last:
        gather_pair(1, hop)
    for k in far:
        mix(0, mb0, top, 0, k)
    ring(1, 3)
    ring(1, 4)
    for hop in last:
        gather_hop(2, hop)
    matmul_whole(0, wo, top)
    finish(xb0, top, 16, xb1.at[me])
    gather_start(3)
    gather_pair(2, 1)
    for k in near:
        mix(0, mb0, low, 1, k)
    first_rest(3)
    ring(3, 0)
    for hop in last:
        gather_pair(2, hop)
    for k in far:
        mix(0, mb0, low, 1, k)
    matmul_whole(0, wo, low)
    finish(xb0, low, 16, xb1.at[me])
    gather_start(4, 0)
    clear_squares((0, r1))
    own_copy(3).wait_recv()
    prepare(1, xb1, top, 0)
    ring(2, 2)
    gather_hop(3, 1, 0)
    gather_start(4, 1)
    gather_hop(3, 1, 1)
    ring(3, 1)
    own_copy(4).wait_recv()
    prepare(1, xb1, low, 0)
    gather_pair(3, 1)
    for k in near:
        prepare(1, xb1, top, k)
    gather_hop(4, 1, 0)
    for hop in last:
        gather_hop(3, hop)
    gather_hop(4, 1, 1)
    for hop in last:
        gather_pair(3, hop)
    for k in far:
        prepare(1, xb1, top, k)
    factors(top)
    for hop in last:
        gather_hop(4, hop)
    gather_pair(4, 1)
    for k in near:
        prepare(1, xb1, low, k)
    ring(2, 3)
    ring(2, 4)
    matmul_whole(1, wag, top)
    gate(top, HALO // 2)
    convolve(1, mb1, (0, cut - HALO))
    stats_send(1, 0)
    gather_start(5)
    ring(3, 2)
    for hop in last:
        gather_pair(4, hop)
    for k in far:
        prepare(1, xb1, low, k)
    matmul_whole(1, wag, low)
    factors(low)
    gate(low, HALO // 2)
    top, low = (0, cut - HALO), (cut - HALO, r2 - cut + HALO)
    convolve(1, mb1, low)
    stats_send(1, 1)
    gather_start(6, 0)
    stats_take(1, 0)
    own_copy(5).wait_recv()
    mix(1, mb1, top, 0, 0)
    gather_hop(5, 1, 0)
    gather_start(6, 1)
    gather_hop(5, 1, 1)
    stats_take(1, 1)
    own_copy(6).wait_recv()
    mix(1, mb1, low, 1, 0)
    gather_hop(6, 1, 0)
    gather_pair(5, 1)
    for k in near:
        mix(1, mb1, top, 0, k)
    ring(3, 3)
    ring(3, 4)
    matmul(1, wo, top, [0])
    matmul(1, wo, top, near)
    for hop in last:
        gather_hop(5, hop)
    gather_hop(6, 1, 1)
    for hop in last:
        gather_pair(5, hop)
    for k in far:
        mix(1, mb1, top, 0, k)
    matmul(1, wo, top, far)
    finish(xb1, top, 16, out)
    for hop in last:
        gather_hop(6, hop)
    gather_pair(6, 1)
    for k in near:
        mix(1, mb1, low, 1, k)
    matmul(1, wo, low, [0])
    matmul(1, wo, low, near)
    for hop in last:
        gather_pair(6, hop)
    for k in far:
        mix(1, mb1, low, 1, k)
    matmul(1, wo, low, far)
    finish(xb1, low, 16, out)

    ring_drain()
    for g in range(7):
        gather_drain(g)
    for c in halo:
        c.wait_send()
    for l in range(2):
        for h in range(2):
            stats_all(l, h).wait_send()
    ln_all.wait_send()


def build(mesh, nz, ny, nx):
    tp = 2 * nx
    spec = (
        P("sp", "tp"), P(), P(None, "sp", "tp"), P(None, "sp", "tp"), P(None, None, "tp"),
        P(None, "tp"), P(None, "tp"), P(None, "tp"), P(None, "sp", "tp"),
    )

    def local(stream, norm_gain, a_w, g_w, conv_w, conv_b, ln_gain, ln_shift, o_w):
        tokens = stream.shape[0]
        width = conv_w.shape[1]
        kb = a_w.shape[1]
        r0, r1, r2 = tokens + 2 * HALO, tokens + HALO, tokens
        lanes = ((r1 // 2 + BLK - 1) // BLK * BLK + 127) // 128 * 128
        dma, f32, b16 = pltpu.SemaphoreType.DMA, jnp.float32, jnp.bfloat16
        hops = max(nz, ny) // 2
        outside = pl.BlockSpec(memory_space=pltpu.HBM)
        return pl.pallas_call(
            functools.partial(kernel, nz, ny, nx, tokens, width),
            out_shape=jax.ShapeDtypeStruct((tokens, C), b16),
            in_specs=[outside] * 9,
            out_specs=pl.BlockSpec(memory_space=pltpu.VMEM),
            scratch_shapes=[
                pltpu.VMEM((2, tp * C), f32),
                pltpu.VMEM((width, 2, C), f32),
                pltpu.VMEM((2, C), f32),
                pltpu.VMEM((2, C), f32),
                pltpu.VMEM((2, C), f32),
                pltpu.VMEM((2, nz, ny, kb, 2 * C), b16),
                pltpu.VMEM((2, nz, ny, kb, C), b16),
                pltpu.VMEM((tp, r0, C), b16),
                pltpu.VMEM((tp, r1, C), b16),
                pltpu.VMEM((tp, r1, C), b16),
                pltpu.VMEM((tp, r2, C), b16),
                pltpu.VMEM((r0, tp * C), b16),
                pltpu.VMEM((2, r0 + BLK, 128), f32),
                pltpu.VMEM((r0, 2 * C), f32),
                pltpu.VMEM((r0, 128), f32),
                pltpu.VMEM((2, lanes, 128), f32),
                pltpu.VMEM((lanes, 128), f32),
                pltpu.VMEM((2, 2, 2, lanes), f32),
                pltpu.VMEM((2, 2, tp, 2, lanes), f32),
                pltpu.VMEM((128, lanes), f32),
                pltpu.VMEM((2, lanes, 128), f32),
                pltpu.VMEM((8, C), f32),
                pltpu.VMEM((tp, 8, C), f32),
                dma((4,)), dma((2, SUB[0])), dma((2, 3)),
                dma((2,)), dma((2, len(ITEMS), 2 * hops - 1)),
                dma((7,)), dma((7, 3 * (nx // 2))), dma((7, nx // 2)), dma((7,)),
                dma((2,)), dma((2,)),
                dma((4,)), dma((4,)),
                dma((1,)), dma((1,)),
                dma((8,)),
            ],
            compiler_params=pltpu.CompilerParams(
                collective_id=0, has_side_effects=True, vmem_limit_bytes=28 * 1024 * 1024
            ),
        )(
            *[pltpu.with_memory_space_constraint(v, pltpu.HBM) for v in (
            stream, a_w, g_w, o_w, norm_gain, jnp.transpose(conv_w, (1, 0, 2)), conv_b, ln_gain, ln_shift,
            )]
        )

    return jax.shard_map(local, mesh=mesh, in_specs=spec, out_specs=P("sp", "tp"), check_vma=False)


def solution(mesh):
    return build(mesh, 8, 8, 4)
```
